32 devices in a mesh: grp: 1, sp: 8 (over z, core), tp: 4 (over y, x).
Axes of the slice: x: 2, y: 2, z: 4, core: 2. Of those that a mesh axis runs over, the one named last changes fastest.
Arguments:
- queries: bfloat16 [2048, 16, 128], P(('grp', 'sp'), 'tp'), may hold values from -6 to 6
- keys: bfloat16 [2048, 4, 128], P(('grp', 'sp'), 'tp'), may hold values from -6 to 6
- values: bfloat16 [2048, 4, 128], P(('grp', 'sp'), 'tp'), may hold values from -6 to 6
- log_gates: float32 [16, 2048], P('tp', ('grp', 'sp')), may hold values from -260 to 0, as said below
- documents: int32 [2048], P(('grp', 'sp')), may hold values from 0 to 2, never falling along the last dimension, each value on 1 to 1536 neighbouring positions
- query_gain: float32 [128], replicated, may hold values from 0.5 to 5
- key_gain: float32 [128], replicated, may hold values from 0.5 to 5
- out_weight: bfloat16 [2048, 2048], P('tp'), may hold values from -0.125 to 0.125
- residual: bfloat16 [2048, 2048], P(('grp', 'sp', 'tp')), may hold values from -1.5 to 1.5
- norm_gain: float32 [2048], replicated, may hold values from 0.1 to 1.9
- routes: int32 [2048, 2], P(('grp', 'sp', 'tp')), may hold values from 0 to 3, all different within a row; in each aligned block of 64 rows (0 to 63, 64 to 127, ...) at most 48 rows name the same one
- route_weights: float32 [2048, 2], P(('grp', 'sp', 'tp')), may hold values from 0.1 to 1
- w_gate: bfloat16 [8, 2048, 2048], P('sp', None, 'tp'), may hold values from -0.125 to 0.125
- w_up: bfloat16 [8, 2048, 2048], P('sp', None, 'tp'), may hold values from -0.125 to 0.125
- w_down: bfloat16 [8, 2048, 2048], P('sp', 'tp'), may hold values from -0.09375 to 0.09375
Outputs:
- layer_out: bfloat16 [2048, 2048], P(('grp', 'sp', 'tp'))
The draws below stay inside these ranges and needn't reach their ends.
Inputs may be any that keep to these rules, and one draw needn't show every extreme that they name: `log_gates`: non-increasing along positions for every head. `documents`: never falls along positions. `routes`: the 2 experts of a token differ; among the 64 tokens of one device (aligned blocks) no expert is named by more than 48 tokens, and in every draw some expert is named by exactly 48 of them.
All inputs are finite; a program needn't handle non-finite values.
Results may differ from the reference program's by a relative error of at most 0.017.
The reference program's roundings to bfloat16 on the way count: a program that leaves them out, or rounds other values in their place, can miss the bound.
Values may be sent and summed in bfloat16 or wider, within the bound.
A program may use at most 128 MiB of HBM per device.

```python
import math
import jax
import jax.numpy as jnp
import numpy as np
from jax import lax

QUERY_HEADS = 16
HEAD_DIM = 128
KV_HEADS = 4
D = 2048
FF_E = 4096
TOK_DEV = 256
DOCS = 3
TOP = 2
SEQUENCE_TOKENS = 2048
ROWS_DEV = 64
EXPERTS = 4
CAP = 48
N_TP = 4


def query_key_pair(key):
    base = jax.random.fold_in(key, 23)
    random_key_list = jax.random.split(base, 2)
    query_draw = jax.random.normal(random_key_list[0], (SEQUENCE_TOKENS, QUERY_HEADS, HEAD_DIM), jnp.float32)
    key_draw = jax.random.normal(random_key_list[1], (SEQUENCE_TOKENS, KV_HEADS, HEAD_DIM), jnp.float32)
    return (jnp.clip(query_draw, -6.0, 6.0), jnp.clip(key_draw, -6.0, 6.0))


def draw_queries(key, part):
    return query_key_pair(key)[0].astype(jnp.bfloat16)


def draw_keys(key, part):
    return query_key_pair(key)[1].astype(jnp.bfloat16)


def draw_values(key, part):
    random_key_list = jax.random.split(jax.random.fold_in(key, 31), 2)
    block_total = SEQUENCE_TOKENS // TOK_DEV
    offsets = jax.random.normal(random_key_list[0], (block_total, KV_HEADS, HEAD_DIM), jnp.float32)
    noise = jax.random.normal(random_key_list[1], (SEQUENCE_TOKENS, KV_HEADS, HEAD_DIM), jnp.float32)
    block_of = jnp.arange(SEQUENCE_TOKENS) // TOK_DEV
    drawn = offsets[block_of] + 0.7 * noise
    return jnp.clip(drawn, -6.0, 6.0).astype(jnp.bfloat16)


def gain_draw(key, salt):
    base = jax.random.fold_in(key, salt)
    return 1.0 + 0.18 * jnp.clip(jax.random.normal(base, (HEAD_DIM,), jnp.float32), -2.5, 2.5)


def draw_query_gain(key, part):
    return gain_draw(key, 41)


def draw_key_gain(key, part):
    return gain_draw(key, 43)


def draw_log_gates(key, part):
    random_key_list = jax.random.split(jax.random.fold_in(key, 11), 7)
    order = jax.random.permutation(random_key_list[0], QUERY_HEADS)
    slower_decay = order < QUERY_HEADS // 2
    fast_rate = jnp.exp(jax.random.uniform(random_key_list[1], (QUERY_HEADS,), jnp.float32, math.log(1.0 / 60.0), math.log(1.0 / 25.0)))
    slow_rate = jnp.exp(jax.random.uniform(random_key_list[2], (QUERY_HEADS,), jnp.float32, math.log(0.05), math.log(0.2))) / SEQUENCE_TOKENS
    rate = jnp.where(slower_decay, slow_rate, fast_rate)
    block_factor = jnp.exp(jax.random.uniform(random_key_list[3], (SEQUENCE_TOKENS // TOK_DEV,), jnp.float32, math.log(0.5), math.log(2.0)))
    token_position = jnp.arange(SEQUENCE_TOKENS)
    spread_factor = jax.random.uniform(random_key_list[4], (QUERY_HEADS, SEQUENCE_TOKENS), jnp.float32, 0.5, 1.5)
    logged_steps = -rate[:, None] * block_factor[token_position // TOK_DEV][None, :] * spread_factor
    surge_position = jax.random.randint(random_key_list[5], (2,), 0, SEQUENCE_TOKENS)
    surge_length = jnp.log(jax.random.uniform(random_key_list[6], (QUERY_HEADS, 2), jnp.float32, 0.5, 0.8))
    routing_hits = (token_position[None, :] == surge_position[:, None]).astype(jnp.float32)
    logged_steps = logged_steps + jnp.where(slower_decay[:, None], jnp.dot(surge_length, routing_hits), 0.0)
    return jnp.cumsum(logged_steps, axis=1)


def steps_of(stream_key, extent, pieces, least, largest):
    level, own = 1.0, jax.random.fold_in(stream_key, 6)
    for position, blocks in pieces:
        steps = jnp.exp(jax.random.uniform(jax.random.fold_in(own, position), (blocks,), jnp.float32, least / len(pieces), largest / len(pieces)))
        level = level * jnp.repeat(steps, extent[position] // blocks).reshape([-1 if axis == position else 1 for axis in range(len(extent))])
    return level


def profile(count, total, limit, slope):
    portions = [(1 << 20) // math.isqrt(grade ** slope) + 1 for grade in range(2, count + 1)]
    spare, holding = total - limit - (count - 1), [1] * (count - 1)
    while spare > 0:
        free = [i for i in range(count - 1) if holding[i] < limit]
        pool, remaining = sum([portions[i] for i in free]), spare
        for i in free:
            extra = min(limit - holding[i], max(1, remaining * portions[i] // pool), spare)
            holding[i] = holding[i] + extra
            spare = spare - extra
    return np.array([limit] + holding)


def uneven(rng, amount, total, limit, skew):
    if amount == 2:
        one = jax.random.randint(rng, (), max(1, total - limit), min(limit, total - 1) + 1)
        return jnp.stack([one, total - one])
    sizes = jnp.asarray(profile(amount, total, limit, skew), jnp.int32)
    twos = (amount - 1) // 2
    source_of, receiver = sizes[1:1 + 2 * twos:2], sizes[2:2 + 2 * twos:2]
    slack = jnp.minimum(source_of - 1, limit - receiver)
    passed = jax.random.randint(jax.random.fold_in(rng, 1), (twos,), 0, 1 << 20) % (slack + 1)
    sizes = sizes.at[1:1 + 2 * twos:2].set(source_of - passed).at[2:2 + 2 * twos:2].set(receiver + passed)
    return sizes[jax.random.permutation(jax.random.fold_in(rng, 2), amount)]


def assign_block(own_key, own, number, rows, number_of, top, bound, slope):
    sequence = jax.random.permutation(own_key, number_of)
    heavy_load, common = load_shares(number_of, rows * top, bound, slope, True), load_shares(number_of, rows * top, bound, slope, False)
    places = jnp.arange(number_of)

    def named(sizes, rotation):
        used = int((sizes > 0).sum())
        fixed = max(1, used // 4)
        shifted = fixed + (places - fixed + rotation * (used - fixed)) % max(1, number_of - fixed)
        return jnp.zeros((number_of,), jnp.int32).at[sequence[jnp.where(places < fixed, places, shifted)]].set(jnp.asarray(sizes, jnp.int32))

    sizes = jnp.where(number % 4 == 0, named(heavy_load, number // 4), named(common, number - number // 4 - 1))
    mixed = jax.random.permutation(jax.random.fold_in(own, 3), number_of)
    donor, receiver = mixed[0:number_of // 2 * 2:2], mixed[1:number_of // 2 * 2:2]
    room = jnp.minimum(sizes[donor] - 1, bound - sizes[receiver]) // 2
    room = jnp.where((donor == sequence[0]) | (receiver == sequence[0]) | (sizes[receiver] == 0), 0, jnp.maximum(room, 0))
    shifted = jax.random.randint(jax.random.fold_in(own, 4), (number_of // 2,), 0, 1 << 20) % (room + 1)
    sizes = sizes.at[donor].add(-shifted).at[receiver].add(shifted)
    items = jnp.searchsorted(jnp.cumsum(sizes), jnp.arange(rows * top), side="right").astype(jnp.int32)
    listing = items.reshape(top, rows).T
    listing = listing[jax.random.permutation(jax.random.fold_in(own, 1), rows)]
    rotation = jax.random.randint(jax.random.fold_in(own, 2), (rows, 1), 0, top)
    return jnp.take_along_axis(listing, (jnp.arange(top)[None, :] + rotation) % top, axis=1)


def load_shares(number_of, total, limit, lean, full):
    weights = [(1 << 20) // math.isqrt(rank ** lean) + 1 for rank in range(1, number_of + 1)]
    largest = limit if full else min(limit, max(-(-total // number_of), total * weights[0] // sum(weights)))
    least = 1 if total - largest >= number_of - 1 else 0
    holding, rest = [largest] + [least] * (number_of - 1), total - largest - least * (number_of - 1)
    while rest > 0:
        candidates = [i for i in range(1, number_of) if holding[i] < largest] or [i for i in range(1, number_of) if holding[i] < limit]
        whole, remaining = sum([weights[i] for i in candidates]), rest
        for i in candidates:
            more = min(limit - holding[i], max(1, remaining * weights[i] // whole), rest)
            holding[i] = holding[i] + more
            rest = rest - more
    return np.array(holding)


def scatter_about(key, dims, spread, most, cuts=(), held_as=jnp.bfloat16):
    level = steps_of(key, dims, cuts, -0.22, 0.18) if cuts else 1.0
    entries = jax.random.normal(key, dims, jnp.float32) * spread * level
    return jnp.minimum(jnp.maximum(entries, -most), most).astype(held_as)


def setup_inputs(seed: int = 0, part: int = 0) -> dict:
    streams_of = jax.random.split(jax.random.key(seed), 16)
    own_keys = jax.random.split(jax.random.fold_in(streams_of[15], part), 16)
    queries = draw_queries(jax.random.fold_in(jax.random.fold_in(streams_of[15], part), 71), part)
    keys = draw_keys(jax.random.fold_in(jax.random.fold_in(streams_of[15], part), 71), part)
    values = draw_values(jax.random.fold_in(jax.random.fold_in(streams_of[15], part), 71), part)
    log_gates = draw_log_gates(jax.random.fold_in(jax.random.fold_in(streams_of[15], part), 71), part)
    documents = jnp.searchsorted(jnp.cumsum(uneven(own_keys[4], DOCS, SEQUENCE_TOKENS, 3 * SEQUENCE_TOKENS // 4, 0)), jnp.arange(SEQUENCE_TOKENS), side="right").astype(jnp.int32)
    query_gain = draw_query_gain(jax.random.fold_in(streams_of[15], 71), part)
    key_gain = draw_key_gain(jax.random.fold_in(streams_of[15], 71), part)
    out_weight = scatter_about(streams_of[7], (D, D), D ** -0.5, 0.125, ((0, 4),))
    residual = scatter_about(own_keys[8], (SEQUENCE_TOKENS, D), 0.25, 1.5, ((0, 32),))
    norm_gain = jnp.clip(1.0 + 0.18 * jax.random.normal(streams_of[9], (D,), jnp.float32), 0.1, 1.9)
    routes_keys = jax.random.split(jax.random.fold_in(own_keys[10], 1), SEQUENCE_TOKENS // ROWS_DEV)
    routes_turns = jax.random.permutation(jax.random.fold_in(own_keys[10], 3), SEQUENCE_TOKENS // ROWS_DEV)
    routes = jax.vmap(lambda own, number: assign_block(jax.random.fold_in(own_keys[10], 2), own, number, ROWS_DEV, EXPERTS, TOP, CAP, 2))(routes_keys, routes_turns).reshape((SEQUENCE_TOKENS, TOP))
    route_weights = jnp.clip(0.1 + 0.9 * jax.random.uniform(own_keys[11], (SEQUENCE_TOKENS, TOP), jnp.float32) ** steps_of(own_keys[11], (SEQUENCE_TOKENS, TOP), ((0, 32),), -0.2, 0.2), 0.1, 1.0)
    w_gate = scatter_about(streams_of[12], (2 * EXPERTS, D, FF_E // 2), D ** -0.5, 0.125, ((0, 8), (2, 4)))
    w_up = scatter_about(streams_of[13], (2 * EXPERTS, D, FF_E // 2), D ** -0.5, 0.125, ((0, 8), (2, 4)))
    w_down = scatter_about(streams_of[14], (2 * EXPERTS, FF_E // 2, D), FF_E ** -0.5, 0.09375, ((0, 8), (1, 4)))
    return dict(queries=queries, keys=keys, values=values, log_gates=log_gates, documents=documents, query_gain=query_gain, key_gain=key_gain, out_weight=out_weight, residual=residual, norm_gain=norm_gain, routes=routes, route_weights=route_weights, w_gate=w_gate, w_up=w_up, w_down=w_down)


EPSILON = 1e-06

def rms_scale(inputs, gain):
    return inputs * lax.rsqrt(lax.optimization_barrier(jnp.mean(inputs * inputs, axis=-1, keepdims=True)) + EPSILON) * gain

def round_trip(array):
    return lax.optimization_barrier(array.astype(jnp.bfloat16)).astype(jnp.float32)

def reference(queries, keys, values, log_gates, documents, query_gain, key_gain, out_weight, residual, norm_gain, routes, route_weights, w_gate, w_up, w_down):
    total_len, head_count, head_size = queries.shape
    kv_count = keys.shape[1]
    group_size = head_count // kv_count
    model_dim = residual.shape[1]
    query_norm = round_trip(rms_scale(queries.astype(jnp.float32), query_gain) * head_size ** (-0.5))
    key_norm = round_trip(rms_scale(keys.astype(jnp.float32), key_gain))
    value_full = values.astype(jnp.float32)
    key_pos = jnp.arange(total_len, dtype=jnp.int32)
    block_rows = 256

    def attend_block(block_index):
        start = block_index * block_rows
        query_block = lax.dynamic_slice_in_dim(query_norm, start, block_rows, 0).reshape(block_rows, kv_count, group_size, head_size)
        scores = jnp.einsum('bkgd,skd->kgbs', query_block, key_norm, precision=lax.Precision.HIGHEST)
        scores = scores.reshape(head_count, block_rows, total_len)
        query_gates = lax.dynamic_slice_in_dim(log_gates, start, block_rows, 1)
        scores = scores + query_gates[:, :, None] - log_gates[:, None, :]
        query_pos = start + jnp.arange(block_rows, dtype=jnp.int32)
        query_docs = lax.dynamic_slice_in_dim(documents, start, block_rows, 0)
        allowed = (key_pos[None, :] <= query_pos[:, None]) & (documents[None, :] == query_docs[:, None])
        scores = jnp.where(allowed[None], scores, -jnp.inf)
        peak = lax.optimization_barrier(jnp.max(scores, axis=-1, keepdims=True))
        expo = jnp.exp(scores - peak)
        denom = lax.optimization_barrier(jnp.sum(expo, axis=-1))
        weights = round_trip(expo).reshape(kv_count, group_size, block_rows, total_len)
        mixed_heads = jnp.einsum('kgbs,skd->bkgd', weights, value_full, precision=lax.Precision.HIGHEST)
        denom_rows = jnp.transpose(denom.reshape(kv_count, group_size, block_rows), (2, 0, 1))
        return (mixed_heads / denom_rows[..., None]).astype(jnp.bfloat16).reshape(block_rows, model_dim)
    attended = lax.map(attend_block, jnp.arange(total_len // block_rows, dtype=jnp.int32)).reshape(total_len, model_dim)
    projected = jnp.dot(attended, out_weight, preferred_element_type=jnp.float32)
    mixed = (residual.astype(jnp.float32) + projected).astype(jnp.bfloat16)
    normed = rms_scale(mixed.astype(jnp.float32), norm_gain).astype(jnp.bfloat16)
    rows_dev = TOK_DEV // N_TP
    block_count = total_len // rows_dev
    slot_count = block_count * CAP
    quarter = FF_E // (2 * N_TP)
    token_ids = jnp.arange(total_len, dtype=jnp.int32)

    def one_expert(summed, expert_index):
        chosen = routes == expert_index
        picked = jnp.any(chosen, axis=1)
        weight = lax.optimization_barrier(jnp.sum(jnp.where(chosen, route_weights, 0.0), axis=1))
        counts = picked.astype(jnp.int32).reshape(block_count, rows_dev)
        rank = (jnp.cumsum(counts, axis=1) - 1).reshape(total_len)
        slot = token_ids // rows_dev * CAP + rank
        slot = jnp.where(picked, slot, slot_count).astype(jnp.int32)
        owner = jnp.zeros((slot_count + 1,), jnp.int32).at[slot].set(token_ids)[:slot_count]
        slot_weight = jnp.zeros((slot_count + 1,), jnp.float32).at[slot].set(weight)[:slot_count]
        rows_in = normed[owner]
        expert_sum = jnp.zeros((slot_count, model_dim), jnp.float32)
        for half in range(2):
            entry = (2 * expert_index + half).astype(jnp.int32)
            gate_all = lax.dynamic_index_in_dim(w_gate, entry, 0, keepdims=False)
            up_all = lax.dynamic_index_in_dim(w_up, entry, 0, keepdims=False)
            down_all = lax.dynamic_index_in_dim(w_down, entry, 0, keepdims=False)
            for column in range(N_TP):
                lower = column * quarter
                gate_act = jnp.dot(rows_in, gate_all[:, lower:lower + quarter], preferred_element_type=jnp.float32)
                up_act = jnp.dot(rows_in, up_all[:, lower:lower + quarter], preferred_element_type=jnp.float32)
                hidden = (jax.nn.silu(gate_act) * up_act).astype(jnp.bfloat16)
                partial_out = jnp.dot(hidden, down_all[lower:lower + quarter, :], preferred_element_type=jnp.float32)
                expert_sum = expert_sum + round_trip(partial_out)
        summed = summed.at[owner].add(slot_weight[:, None] * expert_sum)
        return (summed, None)
    start_sum = jnp.zeros((total_len, model_dim), jnp.float32)
    routed, _ = lax.scan(one_expert, start_sum, jnp.arange(EXPERTS, dtype=jnp.int32))
    return (mixed.astype(jnp.float32) + routed).astype(jnp.bfloat16)
```

```python
import functools

import jax
import jax.numpy as jnp
from jax import lax
from jax.experimental import pallas as pl
from jax.experimental.pallas import tpu as pltpu
from jax.sharding import PartitionSpec as P

EPSILON = 1e-06
CHUNK = 16
LIMBS = 3
MESH = pl.DeviceIdType.MESH
BF16 = jnp.bfloat16
F32 = jnp.float32


def rms_scale(inputs, gain):
    return inputs * lax.rsqrt(jnp.mean(inputs * inputs, axis=-1, keepdims=True) + EPSILON) * gain


def flip(index, bits, size):
    step = 1
    while step < size:
        bit = (bits // step) % 2
        index = index + bit * step * (1 - 2 * ((index // step) % 2))
        step *= 2
    return index


def remote(src, dst, send, recv, where):
    return pltpu.make_async_remote_copy(
        src, dst, send, recv, device_id=where, device_id_type=MESH
    )


def layer_kernel(
    nz,
    n_tp,
    q_ref,
    k_ref,
    v_ref,
    g_ref,
    d_ref,
    qg_ref,
    kg_ref,
    w_hbm,
    res_ref,
    gain_ref,
    rt_ref,
    rw_ref,
    wg_hbm,
    wu_hbm,
    wd_hbm,
    out_ref,
    w_ref,
    wg_ref,
    wu_ref,
    wd_ref,
    qf_ref,
    qt_ref,
    ext_ref,
    kx_ref,
    k_buf,
    v_buf,
    m_ref,
    l_ref,
    acc_ref,
    att_ref,
    sbuf,
    pho_buf,
    prs_buf,
    mixed_ref,
    normed_ref,
    out_buf,
    arrived,
    part,
    hbuf,
    rbuf,
    fin,
    ret,
    w_sem,
    wx_send,
    wx_recv,
    kc_send,
    vc_send,
    kx_send,
    vx_send,
    k_recv,
    v_recv,
    pho_send,
    pho_recv,
    prn_send,
    prn_recv,
    prf_send,
    prf_recv,
    a_send,
    a_recv,
    b_send,
    b_recv,
    f_send,
    f_recv,
    h_send,
    h_recv,
    r_send,
    r_recv,
    z_send,
    z_recv,
):
    s = lax.axis_index("sp")
    t = lax.axis_index("tp")
    z, c = s // 2, s % 2
    heads, rows, hd = acc_ref.shape[0], acc_ref.shape[2], acc_ref.shape[1]
    extra = ext_ref.shape[0]
    cap, width = out_buf.shape[1:]
    share = rows // n_tp
    half = share // 2
    partner = {"sp": 2 * z + 1 - c}
    near = 1 + c
    far = 2 - c
    near_at = flip(t, near, n_tp)
    far_at = flip(t, far, n_tp)
    to_near = {"tp": near_at}
    to_far = {"tp": far_at}

    barrier = pltpu.get_barrier_semaphore()
    for dz in range(1, nz):
        pl.semaphore_signal(
            barrier, inc=1, device_id={"sp": 2 * ((z + dz) % nz) + c}, device_id_type=MESH
        )
    for k in (1, 2):
        pl.semaphore_signal(
            barrier, inc=1, device_id={"tp": flip(t, k, n_tp)}, device_id_type=MESH
        )
    pl.semaphore_signal(barrier, inc=1, device_id=partner, device_id_type=MESH)
    loads = [
        pltpu.make_async_copy(src, dst, w_sem.at[i])
        for i, (src, dst) in enumerate(
            (
                (w_hbm, w_ref),
                (wg_hbm, wg_ref.at[0]),
                (wu_hbm, wu_ref.at[0]),
                (wd_hbm, wd_ref.at[0]),
            )
        )
    ]
    for load in loads:
        load.start()
    swaps = [
        remote(src, dst, wx_send.at[i], wx_recv.at[i], partner)
        for i, (src, dst) in enumerate(
            ((wg_hbm, wg_ref.at[1]), (wu_hbm, wu_ref.at[1]), (wd_hbm, wd_ref.at[1]))
        )
    ]

    k_buf[s] = rms_scale(k_ref[...].astype(F32), kg_ref[...]).astype(BF16)
    v_buf[s, 0:hd, :] = jnp.transpose(v_ref[...].astype(F32)).astype(BF16)
    gates = -g_ref[...]
    high = gates.astype(BF16).astype(F32)
    middle = (gates - high).astype(BF16).astype(F32)
    low = (gates - high - middle).astype(BF16).astype(F32)
    limbs = (high, middle, low)
    ext_ref[...] = jnp.zeros_like(ext_ref)
    for j, limb in enumerate(limbs):
        ext_ref[j * heads:(j + 1) * heads, :] = limb
    ones_at = LIMBS * heads
    doc_at = ones_at + LIMBS
    ext_ref[ones_at:ones_at + LIMBS, :] = jnp.ones((LIMBS, rows), F32)
    ext_ref[doc_at:doc_at + 1, :] = d_ref[...].astype(F32)
    v_buf[s, hd:hd + extra, :] = ext_ref[...].astype(BF16)

    pl.semaphore_wait(barrier, nz - 1 + 2 + 1)

    def chain(source, slot):
        there = {"sp": 2 * (z + 1) + c}
        return (
            remote(
                k_buf.at[source], k_buf.at[source], kc_send.at[slot], k_recv.at[source], there
            ),
            remote(
                v_buf.at[source], v_buf.at[source], vc_send.at[slot], v_recv.at[source], there
            ),
        )

    def across(source, slot):
        return (
            remote(
                k_buf.at[source], k_buf.at[source], kx_send.at[slot], k_recv.at[source], partner
            ),
            remote(
                v_buf.at[source], v_buf.at[source], vx_send.at[slot], v_recv.at[source], partner
            ),
        )

    @pl.when(z + 1 < nz)
    def _():
        for copy in chain(s, 0):
            copy.start()

    @pl.when(c == 0)
    def _():
        for copy in across(s, 0):
            copy.start()

    qf_ref[...] = q_ref[...].astype(F32)
    row = lax.broadcasted_iota(jnp.int32, (extra, rows), 0)
    for h in range(heads):
        picked = qf_ref[pl.ds(h, rows, stride=heads), :]
        query = (rms_scale(picked, qg_ref[...]) * hd ** (-0.5)).astype(BF16).astype(F32)
        qt_ref[h, 0:hd, :] = jnp.transpose(query).astype(BF16)
        mine = jnp.where((row < ones_at) & (row % heads == h), 1.0, 0.0)
        for j, limb in enumerate(limbs):
            mine = jnp.where(row == ones_at + j, -limb[h:h + 1, :], mine)
        qt_ref[h, hd:hd + extra, :] = mine.astype(BF16)
        qt_ref[h, hd + extra:, :] = jnp.zeros((hd - extra, rows), BF16)
    kx_ref[...] = jnp.zeros_like(kx_ref)
    here = d_ref[...].astype(F32)

    def update(source, own):
        kx_ref[0:extra, :] = v_buf[source, hd:hd + extra, :].astype(F32)
        columns = jnp.transpose(kx_ref[...])
        left = jnp.concatenate([k_buf[source], columns.astype(BF16)], axis=1)
        same = columns[:, doc_at:doc_at + 1] == here
        if own:
            key_at = lax.broadcasted_iota(jnp.int32, (rows, rows), 0)
            query_at = lax.broadcasted_iota(jnp.int32, (rows, rows), 1)
            same = same & (key_at <= query_at)
        for h in range(heads):
            scores = jnp.dot(left, qt_ref[h], preferred_element_type=F32)
            scores = jnp.where(same, scores, -jnp.inf)
            peak = jnp.max(scores, axis=0, keepdims=True)
            if own:
                new = peak
            else:
                old = m_ref[h]
                new = jnp.maximum(old, peak)
            expo = jnp.exp(scores - new)
            total = jnp.sum(expo, axis=0, keepdims=True)
            mix = jnp.dot(
                v_buf[source, 0:hd, :], expo.astype(BF16), preferred_element_type=F32
            )
            m_ref[h] = new
            if own:
                l_ref[h] = total
                acc_ref[h] = mix
            else:
                factor = jnp.exp(old - new)
                l_ref[h] = factor * l_ref[h] + total
                acc_ref[h] = factor * acc_ref[h] + mix

    update(s, True)

    def one_source(i, carry):
        dz = (i + 1) // 2
        direct = i % 2
        core = (1 - direct) * (1 - c) + direct * c
        source = 2 * (z - dz) + core
        for copy in across(source, dz):
            copy.wait_recv()

        @pl.when(direct == 1)
        def _():
            @pl.when(z + 1 < nz)
            def _():
                for copy in chain(source, dz):
                    copy.start()

            for copy in across(source, dz):
                copy.start()

        update(source, False)
        return carry

    lax.fori_loop(1 - c, 2 * z + 1, one_source, 0)

    for swap in swaps:
        swap.start()

    for h in range(heads):
        att_ref[:, h * hd:(h + 1) * hd] = jnp.transpose(acc_ref[h] / l_ref[h]).astype(BF16)

    def ho_copy(i):
        return remote(
            sbuf.at[3, pl.ds(i * half, half)], pho_buf.at[i], pho_send.at[i], pho_recv.at[i],
            to_near,
        )

    def rn_copy(i):
        return remote(
            sbuf.at[near, pl.ds(i * half, half)], prs_buf.at[0, pl.ds(i * half, half)],
            prn_send.at[i], prn_recv.at[i], to_near,
        )

    def rf_copy(i):
        return remote(
            sbuf.at[far, pl.ds(i * half, half)], prs_buf.at[1, pl.ds(i * half, half)],
            prf_send.at[i], prf_recv.at[i], to_far,
        )

    loads[0].wait()

    def project(k, column):
        start = pl.multiple_of(column * share, share)
        block = jnp.dot(
            att_ref[pl.ds(start, share), :], w_ref[...], preferred_element_type=F32
        )
        sbuf[k] = block.astype(BF16)

    def project_step(i, carry):
        k = (i == 0) * 3 + (i == 1) * near + (i == 2) * far
        project(k, flip(t, k, n_tp))

        @pl.when(i == 0)
        def _():
            for j in range(2):
                ho_copy(j).start()

        @pl.when(i == 1)
        def _():
            for j in range(2):
                rn_copy(j).start()

        return carry

    lax.fori_loop(0, n_tp, project_step, 0)

    for i in range(2):
        ho_copy(i).wait_recv()

        def pair(r, carry, i=i):
            at = pl.ds(pl.multiple_of(i * half + r * CHUNK, CHUNK), CHUNK)
            here_at = pl.ds(pl.multiple_of(r * CHUNK, CHUNK), CHUNK)
            total = sbuf[far, at, :].astype(F32) + pho_buf[i, here_at, :].astype(F32)
            sbuf[far, at, :] = total.astype(BF16)
            return carry

        lax.fori_loop(0, half // CHUNK, pair, 0)
        rf_copy(i).start()

    experts = nz
    padded = experts + (-experts) % 8
    n_slots = experts * cap
    first, second = rt_ref[0:1, :], rt_ref[1:2, :]
    names = lax.broadcasted_iota(jnp.int32, (padded, share), 0)
    chosen = [(names == first).astype(F32), (names == second).astype(F32)]
    up_to = lax.broadcasted_iota(jnp.int32, (share, share), 0) <= lax.broadcasted_iota(
        jnp.int32, (share, share), 1
    )
    rank = (
        jnp.dot(
            (chosen[0] + chosen[1]).astype(BF16),
            up_to.astype(F32).astype(BF16),
            preferred_element_type=F32,
        )
        - 1.0
    )
    start_of = names.astype(F32) * cap
    slots = [
        jnp.sum(choice * (rank + start_of), axis=0, keepdims=True) for choice in chosen
    ]
    slot_rows = lax.broadcasted_iota(jnp.int32, (n_slots, share), 0).astype(F32)
    placing = (
        (slot_rows == slots[0]).astype(F32) + (slot_rows == slots[1]).astype(F32)
    ).astype(BF16)
    diagonal = (
        lax.broadcasted_iota(jnp.int32, (share, share), 0)
        == lax.broadcasted_iota(jnp.int32, (share, share), 1)
    ).astype(F32)

    def column(values):
        return jnp.sum(diagonal * values, axis=1, keepdims=True)

    slot_columns = lax.broadcasted_iota(jnp.int32, (share, n_slots), 1).astype(F32)
    taking = [(slot_columns == column(slot)).astype(F32).astype(BF16) for slot in slots]
    weights = [column(rw_ref[k:k + 1, :]) for k in range(2)]

    for i in range(2):
        rn_copy(i).wait_recv()
        rf_copy(i).wait_recv()

        def finish(r, carry, i=i):
            at = pl.ds(pl.multiple_of(i * half + r * CHUNK, CHUNK), CHUNK)
            total = (
                sbuf[0, at, :].astype(F32)
                + prs_buf[0, at, :].astype(F32)
                + prs_buf[1, at, :].astype(F32)
            )
            mixed = (res_ref[at, :].astype(F32) + total).astype(BF16)
            mixed_ref[at, :] = mixed
            normed_ref[at, :] = rms_scale(mixed.astype(F32), gain_ref[...]).astype(BF16)
            return carry

        lax.fori_loop(0, half // CHUNK, finish, 0)

    out_buf[...] = (
        jnp.dot(placing, normed_ref[...], preferred_element_type=F32)
        .astype(BF16)
        .reshape(experts, cap, width)
    )

    def order(j):
        return j

    def along(e):
        return remote(
            out_buf.at[e], arrived.at[z, t], a_send.at[e], a_recv.at[z], {"sp": 2 * e + c}
        )

    def along_in(p):
        return remote(
            arrived.at[p, t], arrived.at[p, t], a_send.at[p], a_recv.at[p], partner
        )

    def spread(p, k):
        block = arrived.at[p, t]
        return remote(
            block, block, b_send.at[k, p], b_recv.at[k, p], to_far if k else to_near
        )

    def spread_in(p, k):
        block = arrived.at[p, far_at if k else near_at]
        return remote(block, block, b_send.at[k, p], b_recv.at[k, p], partner)

    def forward(p):
        block = arrived.at[p, far_at]
        return remote(block, block, f_send.at[p], f_recv.at[p], to_near)

    def forward_in(p):
        block = arrived.at[p, flip(t, 3, n_tp)]
        return remote(block, block, f_send.at[p], f_recv.at[p], partner)

    def hand_over(p):
        return remote(
            part.at[p, flip(t, 3, n_tp)], hbuf.at[p], h_send.at[p], h_recv.at[p], to_near
        )

    def reduce_near(p):
        return remote(
            part.at[p, near_at], rbuf.at[p, 0], r_send.at[0, p], r_recv.at[0, p], to_near
        )

    def reduce_far(p):
        return remote(
            part.at[p, far_at], rbuf.at[p, 1], r_send.at[1, p], r_recv.at[1, p], to_far
        )

    def home(p):
        return remote(
            fin.at[p], ret.at[z], z_send.at[p], z_recv.at[z], {"sp": 2 * p + c}
        )

    def home_in(e):
        return remote(fin.at[e], ret.at[e], z_send.at[e], z_recv.at[e], partner)

    def launch(p):
        @pl.when(p != z)
        def _():
            along_in(p).wait_recv()

        spread(p, 0).start()
        spread(p, 1).start()

    arrived[z, t] = out_buf[z]

    def send_out(dz, carry):
        along((z + dz) % nz).start()
        return carry

    lax.fori_loop(1, nz, send_out, 0)
    launch(order(0))
    for load in loads[1:]:
        load.wait()
    for swap in swaps:
        swap.wait_recv()

    def step(j, carry):
        @pl.when(j < nz)
        def _():
            p = order(j)
            spread_in(p, 1).wait_recv()
            forward(p).start()

        @pl.when(j + 1 < nz)
        def _():
            launch(order(j + 1))

        @pl.when((j >= 1) & (j <= nz))
        def _():
            p = order(j - 1)
            hand_over(p).wait_recv()

            def one(r, carry):
                at = pl.ds(pl.multiple_of(r * CHUNK, CHUNK), CHUNK)
                total = part[p, far_at, at, :].astype(F32) + hbuf[p, at, :].astype(F32)
                part[p, far_at, at, :] = total.astype(BF16)
                return carry

            lax.fori_loop(0, cap // CHUNK, one, 0)
            reduce_far(p).start()

        @pl.when(j < nz)
        def _():
            p = order(j)
            spread_in(p, 0).wait_recv()
            forward_in(p).wait_recv()
            flat = arrived[p].reshape(n_tp * cap, width)
            result = None
            for i in range(2):
                gate = jnp.dot(flat, wg_ref[i], preferred_element_type=F32)
                up = jnp.dot(flat, wu_ref[i], preferred_element_type=F32)
                hidden = (gate * (1.0 / (1.0 + jnp.exp(-gate))) * up).astype(BF16)
                down = jnp.dot(hidden, wd_ref[i], preferred_element_type=F32)
                result = down if result is None else result + down
            part[p] = result.astype(BF16).reshape(n_tp, cap, width)
            hand_over(p).start()
            reduce_near(p).start()

        @pl.when((j >= 2) & (j - 2 < nz))
        def _():
            p = order(j - 2)
            reduce_near(p).wait_recv()
            reduce_far(p).wait_recv()

            def one(r, carry):
                at = pl.ds(pl.multiple_of(r * CHUNK, CHUNK), CHUNK)
                total = (
                    part[p, t, at, :].astype(F32)
                    + rbuf[p, 0, at, :].astype(F32)
                    + rbuf[p, 1, at, :].astype(F32)
                )
                fin[p, at, :] = total.astype(BF16)
                return carry

            lax.fori_loop(0, cap // CHUNK, one, 0)

            @pl.when(p != z)
            def _():
                home(p).start()

            @pl.when(p == z)
            def _():
                ret[z] = fin[z]

        return carry

    lax.fori_loop(0, nz + 2, step, 0)

    def collect(dz, carry):
        home_in((z + dz) % nz).wait_recv()
        return carry

    lax.fori_loop(1, nz, collect, 0)

    both = jnp.concatenate(taking, axis=0)
    piece = width // 4
    for i in range(4):
        at = slice(i * piece, (i + 1) * piece)
        back = ret[:, :, at].reshape(n_slots, piece)
        rows_of = jnp.dot(both, back, preferred_element_type=F32)
        routed = weights[0] * rows_of[:share] + weights[1] * rows_of[share:]
        out_ref[:, at] = (mixed_ref[:, at].astype(F32) + routed).astype(BF16)

    def sent(dz, carry):
        p = (z + dz) % nz
        home(p).wait_send()
        along(p).wait_send()
        return carry

    lax.fori_loop(1, nz, sent, 0)

    def sent_plane(p, carry):
        for k in range(2):
            spread(p, k).wait_send()
        forward(p).wait_send()
        hand_over(p).wait_send()
        reduce_near(p).wait_send()
        reduce_far(p).wait_send()
        return carry

    lax.fori_loop(0, nz, sent_plane, 0)
    for i in range(2):
        ho_copy(i).wait_send()
        rn_copy(i).wait_send()
        rf_copy(i).wait_send()
    for swap in swaps:
        swap.wait_send()

    @pl.when(c == 0)
    def _():
        for copy in across(s, 0):
            copy.wait_send()

    @pl.when(z + 1 < nz)
    def _():
        for copy in chain(s, 0):
            copy.wait_send()

    def sent_source(dz, carry):
        source = 2 * (z - dz) + c
        for copy in across(source, dz):
            copy.wait_send()

        @pl.when(z + 1 < nz)
        def _():
            for copy in chain(source, dz):
                copy.wait_send()

        return carry

    lax.fori_loop(1, z + 1, sent_source, 0)


def local(
    nz,
    n_tp,
    queries,
    keys,
    values,
    log_gates,
    documents,
    query_gain,
    key_gain,
    out_weight,
    residual,
    norm_gain,
    routes,
    route_weights,
    w_gate,
    w_up,
    w_down,
):
    tok_dev, heads, hd = queries.shape
    rows_dev, width = residual.shape
    n_sp = 2 * nz
    named = min(rows_dev, 6 * rows_dev // n_sp)
    cap = named + (-named) % CHUNK
    hidden_dev = w_gate.shape[2]
    extra = LIMBS * heads + LIMBS + 1
    extra = extra + (-extra) % 16
    vmem = pl.BlockSpec(memory_space=pltpu.VMEM)
    hbm = pl.BlockSpec(memory_space=pl.ANY)
    dma = pltpu.SemaphoreType.DMA
    block = (cap, width)
    return pl.pallas_call(
        functools.partial(layer_kernel, nz, n_tp),
        out_shape=jax.ShapeDtypeStruct((rows_dev, width), BF16),
        in_specs=[vmem] * 7 + [hbm] + [vmem] * 4 + [hbm] * 3,
        out_specs=vmem,
        scratch_shapes=[
            pltpu.VMEM(out_weight.shape, BF16),
            pltpu.VMEM((2, width, hidden_dev), BF16),
            pltpu.VMEM((2, width, hidden_dev), BF16),
            pltpu.VMEM((2, hidden_dev, width), BF16),
            pltpu.VMEM((tok_dev * heads, hd), F32),
            pltpu.VMEM((heads, 2 * hd, tok_dev), BF16),
            pltpu.VMEM((extra, tok_dev), F32),
            pltpu.VMEM((hd, tok_dev), F32),
            pltpu.VMEM((n_sp, tok_dev, hd), BF16),
            pltpu.VMEM((n_sp, hd + extra, tok_dev), BF16),
            pltpu.VMEM((heads, 1, tok_dev), F32),
            pltpu.VMEM((heads, 1, tok_dev), F32),
            pltpu.VMEM((heads, hd, tok_dev), F32),
            pltpu.VMEM((tok_dev, heads * hd), BF16),
            pltpu.VMEM((n_tp, rows_dev, width), BF16),
            pltpu.VMEM((2, rows_dev // 2, width), BF16),
            pltpu.VMEM((2, rows_dev, width), BF16),
            pltpu.VMEM((rows_dev, width), BF16),
            pltpu.VMEM((rows_dev, width), BF16),
            pltpu.VMEM((nz,) + block, BF16),
            pltpu.VMEM((nz, n_tp) + block, BF16),
            pltpu.VMEM((nz, n_tp) + block, BF16),
            pltpu.VMEM((nz,) + block, BF16),
            pltpu.VMEM((nz, 2) + block, BF16),
            pltpu.VMEM((nz,) + block, BF16),
            pltpu.VMEM((nz,) + block, BF16),
            dma((4,)),
            dma((3,)),
            dma((3,)),
            dma((nz,)),
            dma((nz,)),
            dma((nz,)),
            dma((nz,)),
            dma((n_sp,)),
            dma((n_sp,)),
            dma((2,)),
            dma((2,)),
            dma((2,)),
            dma((2,)),
            dma((2,)),
            dma((2,)),
            dma((nz,)),
            dma((nz,)),
            dma((2, nz)),
            dma((2, nz)),
            dma((nz,)),
            dma((nz,)),
            dma((nz,)),
            dma((nz,)),
            dma((2, nz)),
            dma((2, nz)),
            dma((nz,)),
            dma((nz,)),
        ],
        compiler_params=pltpu.CompilerParams(
            collective_id=0, has_side_effects=True, vmem_limit_bytes=60 * 1024 * 1024
        ),
        name="layer",
    )(
        queries.reshape(tok_dev * heads, hd),
        keys.reshape(tok_dev, hd),
        values.reshape(tok_dev, hd),
        log_gates,
        documents[None, :],
        query_gain[None, :],
        key_gain[None, :],
        out_weight,
        residual,
        norm_gain[None, :],
        routes.T,
        route_weights.T,
        w_gate[0],
        w_up[0],
        w_down[0],
    )


def solution(mesh):
    return jax.shard_map(
        functools.partial(local, mesh.shape["sp"] // 2, mesh.shape["tp"]),
        mesh=mesh,
        in_specs=(
            P(("grp", "sp"), "tp", None),
            P(("grp", "sp"), "tp", None),
            P(("grp", "sp"), "tp", None),
            P("tp", ("grp", "sp")),
            P(("grp", "sp")),
            P(),
            P(),
            P("tp", None),
            P(("grp", "sp", "tp"), None),
            P(),
            P(("grp", "sp", "tp"), None),
            P(("grp", "sp", "tp"), None),
            P("sp", None, "tp"),
            P("sp", None, "tp"),
            P("sp", "tp", None),
        ),
        out_specs=P(("grp", "sp", "tp"), None),
        check_vma=False,
    )
```

```python
import functools

import jax
import jax.numpy as jnp
from jax import lax
from jax.experimental import pallas as pl
from jax.experimental.pallas import tpu as pltpu
from jax.sharding import PartitionSpec as P

EPSILON = 1e-06
CHUNK = 16
LIMBS = 3
MESH = pl.DeviceIdType.MESH
BF16 = jnp.bfloat16
F32 = jnp.float32


def rms_scale(inputs, gain):
    return inputs * lax.rsqrt(jnp.mean(inputs * inputs, axis=-1, keepdims=True) + EPSILON) * gain


def flip(index, bits, size):
    step = 1
    while step < size:
        bit = (bits // step) % 2
        index = index + bit * step * (1 - 2 * ((index // step) % 2))
        step *= 2
    return index


def remote(src, dst, send, recv, where):
    return pltpu.make_async_remote_copy(
        src, dst, send, recv, device_id=where, device_id_type=MESH
    )


def layer_kernel(
    nz,
    n_tp,
    q_ref,
    k_ref,
    v_ref,
    g_ref,
    d_ref,
    qg_ref,
    kg_ref,
    w_hbm,
    res_ref,
    gain_ref,
    rt_ref,
    rw_ref,
    wg_hbm,
    wu_hbm,
    wd_hbm,
    out_ref,
    w_ref,
    wg_ref,
    wu_ref,
    wd_ref,
    qf_ref,
    qt_ref,
    ext_ref,
    kx_ref,
    k_buf,
    v_buf,
    m_ref,
    l_ref,
    acc_ref,
    att_ref,
    sbuf,
    pho_buf,
    prs_buf,
    mixed_ref,
    normed_ref,
    out_buf,
    arrived,
    part,
    hbuf,
    rbuf,
    fin,
    ret,
    w_sem,
    wx_send,
    wx_recv,
    kc_send,
    vc_send,
    kx_send,
    vx_send,
    k_recv,
    v_recv,
    pho_send,
    pho_recv,
    prn_send,
    prn_recv,
    prf_send,
    prf_recv,
    a_send,
    a_recv,
    b_send,
    b_recv,
    f_send,
    f_recv,
    h_send,
    h_recv,
    r_send,
    r_recv,
    z_send,
    z_recv,
):
    s = lax.axis_index("sp")
    t = lax.axis_index("tp")
    z, c = s // 2, s % 2
    heads, rows, hd = acc_ref.shape[0], acc_ref.shape[2], acc_ref.shape[1]
    extra = ext_ref.shape[0]
    cap, width = out_buf.shape[1:]
    share = rows // n_tp
    half = share // 2
    partner = {"sp": 2 * z + 1 - c}
    near = 1 + c
    far = 2 - c
    near_at = flip(t, near, n_tp)
    far_at = flip(t, far, n_tp)
    to_near = {"tp": near_at}
    to_far = {"tp": far_at}

    barrier = pltpu.get_barrier_semaphore()
    for dz in range(1, nz):
        pl.semaphore_signal(
            barrier, inc=1, device_id={"sp": 2 * ((z + dz) % nz) + c}, device_id_type=MESH
        )
    for k in (1, 2):
        pl.semaphore_signal(
            barrier, inc=1, device_id={"tp": flip(t, k, n_tp)}, device_id_type=MESH
        )
    pl.semaphore_signal(barrier, inc=1, device_id=partner, device_id_type=MESH)
    loads = [
        pltpu.make_async_copy(src, dst, w_sem.at[i])
        for i, (src, dst) in enumerate(
            (
                (w_hbm, w_ref),
                (wg_hbm, wg_ref.at[0]),
                (wu_hbm, wu_ref.at[0]),
                (wd_hbm, wd_ref.at[0]),
            )
        )
    ]
    for load in loads:
        load.start()
    swaps = [
        remote(src, dst, wx_send.at[i], wx_recv.at[i], partner)
        for i, (src, dst) in enumerate(
            ((wg_hbm, wg_ref.at[1]), (wu_hbm, wu_ref.at[1]), (wd_hbm, wd_ref.at[1]))
        )
    ]

    k_buf[s] = rms_scale(k_ref[...].astype(F32), kg_ref[...]).astype(BF16)
    v_buf[s, 0:hd, :] = jnp.transpose(v_ref[...].astype(F32)).astype(BF16)
    gates = -g_ref[...]
    high = gates.astype(BF16).astype(F32)
    middle = (gates - high).astype(BF16).astype(F32)
    low = (gates - high - middle).astype(BF16).astype(F32)
    limbs = (high, middle, low)
    ext_ref[...] = jnp.zeros_like(ext_ref)
    for j, limb in enumerate(limbs):
        ext_ref[j * heads:(j + 1) * heads, :] = limb
    ones_at = LIMBS * heads
    doc_at = ones_at + LIMBS
    ext_ref[ones_at:ones_at + LIMBS, :] = jnp.ones((LIMBS, rows), F32)
    ext_ref[doc_at:doc_at + 1, :] = d_ref[...].astype(F32)
    v_buf[s, hd:hd + extra, :] = ext_ref[...].astype(BF16)

    pl.semaphore_wait(barrier, nz - 1 + 2 + 1)

    def chain(source, slot):
        there = {"sp": 2 * (z + 1) + c}
        return (
            remote(
                k_buf.at[source], k_buf.at[source], kc_send.at[slot], k_recv.at[source], there
            ),
            remote(
                v_buf.at[source], v_buf.at[source], vc_send.at[slot], v_recv.at[source], there
            ),
        )

    def across(source, slot):
        return (
            remote(
                k_buf.at[source], k_buf.at[source], kx_send.at[slot], k_recv.at[source], partner
            ),
            remote(
                v_buf.at[source], v_buf.at[source], vx_send.at[slot], v_recv.at[source], partner
            ),
        )

    @pl.when(z + 1 < nz)
    def _():
        for copy in chain(s, 0):
            copy.start()

    @pl.when(c == 0)
    def _():
        for copy in across(s, 0):
            copy.start()

    qf_ref[...] = q_ref[...].astype(F32)
    row = lax.broadcasted_iota(jnp.int32, (extra, rows), 0)
    for h in range(heads):
        picked = qf_ref[pl.ds(h, rows, stride=heads), :]
        query = (rms_scale(picked, qg_ref[...]) * hd ** (-0.5)).astype(BF16).astype(F32)
        qt_ref[h, 0:hd, :] = jnp.transpose(query).astype(BF16)
        mine = jnp.where((row < ones_at) & (row % heads == h), 1.0, 0.0)
        for j, limb in enumerate(limbs):
            mine = jnp.where(row == ones_at + j, -limb[h:h + 1, :], mine)
        qt_ref[h, hd:hd + extra, :] = mine.astype(BF16)
        qt_ref[h, hd + extra:, :] = jnp.zeros((hd - extra, rows), BF16)
    kx_ref[...] = jnp.zeros_like(kx_ref)
    here = d_ref[...].astype(F32)

    def update(source, own):
        kx_ref[0:extra, :] = v_buf[source, hd:hd + extra, :].astype(F32)
        columns = jnp.transpose(kx_ref[...])
        left = jnp.concatenate([k_buf[source], columns.astype(BF16)], axis=1)
        same = columns[:, doc_at:doc_at + 1] == here
        if own:
            key_at = lax.broadcasted_iota(jnp.int32, (rows, rows), 0)
            query_at = lax.broadcasted_iota(jnp.int32, (rows, rows), 1)
            same = same & (key_at <= query_at)
        for h in range(heads):
            scores = jnp.dot(left, qt_ref[h], preferred_element_type=F32)
            scores = jnp.where(same, scores, -jnp.inf)
            peak = jnp.max(scores, axis=0, keepdims=True)
            if own:
                new = peak
            else:
                old = m_ref[h]
                new = jnp.maximum(old, peak)
            expo = jnp.exp(scores - new)
            total = jnp.sum(expo, axis=0, keepdims=True)
            mix = jnp.dot(
                v_buf[source, 0:hd, :], expo.astype(BF16), preferred_element_type=F32
            )
            m_ref[h] = new
            if own:
                l_ref[h] = total
                acc_ref[h] = mix
            else:
                factor = jnp.exp(old - new)
                l_ref[h] = factor * l_ref[h] + total
                acc_ref[h] = factor * acc_ref[h] + mix

    update(s, True)

    def one_source(i, carry):
        dz = (i + 1) // 2
        direct = i % 2
        core = (1 - direct) * (1 - c) + direct * c
        source = 2 * (z - dz) + core
        onward = chain(source, dz)
        aside = across(source, dz)
        for k in range(2):
            aside[k].wait_recv()

            @pl.when(direct == 1)
            def _(k=k):
                @pl.when(z + 1 < nz)
                def _():
                    onward[k].start()

                aside[k].start()

        update(source, False)
        return carry

    lax.fori_loop(1 - c, 2 * z + 1, one_source, 0)

    for swap in swaps:
        swap.start()

    for h in range(heads):
        att_ref[:, h * hd:(h + 1) * hd] = jnp.transpose(acc_ref[h] / l_ref[h]).astype(BF16)

    def ho_copy(i):
        return remote(
            sbuf.at[3, pl.ds(i * half, half)], pho_buf.at[i], pho_send.at[i], pho_recv.at[i],
            to_near,
        )

    def rn_copy(i):
        return remote(
            sbuf.at[near, pl.ds(i * half, half)], prs_buf.at[0, pl.ds(i * half, half)],
            prn_send.at[i], prn_recv.at[i], to_near,
        )

    def rf_copy(i):
        return remote(
            sbuf.at[far, pl.ds(i * half, half)], prs_buf.at[1, pl.ds(i * half, half)],
            prf_send.at[i], prf_recv.at[i], to_far,
        )

    loads[0].wait()

    def project(k, column):
        start = pl.multiple_of(column * share, share)
        block = jnp.dot(
            att_ref[pl.ds(start, share), :], w_ref[...], preferred_element_type=F32
        )
        sbuf[k] = block.astype(BF16)

    def project_step(i, carry):
        k = (i == 0) * 3 + (i == 1) * near + (i == 2) * far
        project(k, flip(t, k, n_tp))

        @pl.when(i == 0)
        def _():
            for j in range(2):
                ho_copy(j).start()

        @pl.when(i == 1)
        def _():
            for j in range(2):
                rn_copy(j).start()

        return carry

    lax.fori_loop(0, n_tp, project_step, 0)

    for i in range(2):
        ho_copy(i).wait_recv()

        def pair(r, carry, i=i):
            at = pl.ds(pl.multiple_of(i * half + r * CHUNK, CHUNK), CHUNK)
            here_at = pl.ds(pl.multiple_of(r * CHUNK, CHUNK), CHUNK)
            total = sbuf[far, at, :].astype(F32) + pho_buf[i, here_at, :].astype(F32)
            sbuf[far, at, :] = total.astype(BF16)
            return carry

        lax.fori_loop(0, half // CHUNK, pair, 0)
        rf_copy(i).start()

    experts = nz
    padded = experts + (-experts) % 8
    n_slots = experts * cap
    first, second = rt_ref[0:1, :], rt_ref[1:2, :]
    names = lax.broadcasted_iota(jnp.int32, (padded, share), 0)
    chosen = [(names == first).astype(F32), (names == second).astype(F32)]
    up_to = lax.broadcasted_iota(jnp.int32, (share, share), 0) <= lax.broadcasted_iota(
        jnp.int32, (share, share), 1
    )
    rank = (
        jnp.dot(
            (chosen[0] + chosen[1]).astype(BF16),
            up_to.astype(F32).astype(BF16),
            preferred_element_type=F32,
        )
        - 1.0
    )
    start_of = names.astype(F32) * cap
    slots = [
        jnp.sum(choice * (rank + start_of), axis=0, keepdims=True) for choice in chosen
    ]
    slot_rows = lax.broadcasted_iota(jnp.int32, (n_slots, share), 0).astype(F32)
    placing = (
        (slot_rows == slots[0]).astype(F32) + (slot_rows == slots[1]).astype(F32)
    ).astype(BF16)
    diagonal = (
        lax.broadcasted_iota(jnp.int32, (share, share), 0)
        == lax.broadcasted_iota(jnp.int32, (share, share), 1)
    ).astype(F32)

    def column(values):
        return jnp.sum(diagonal * values, axis=1, keepdims=True)

    slot_columns = lax.broadcasted_iota(jnp.int32, (share, n_slots), 1).astype(F32)
    taking = [(slot_columns == column(slot)).astype(F32).astype(BF16) for slot in slots]
    weights = [column(rw_ref[k:k + 1, :]) for k in range(2)]

    for i in range(2):
        rn_copy(i).wait_recv()
        rf_copy(i).wait_recv()

        def finish(r, carry, i=i):
            at = pl.ds(pl.multiple_of(i * half + r * CHUNK, CHUNK), CHUNK)
            total = (
                sbuf[0, at, :].astype(F32)
                + prs_buf[0, at, :].astype(F32)
                + prs_buf[1, at, :].astype(F32)
            )
            mixed = (res_ref[at, :].astype(F32) + total).astype(BF16)
            mixed_ref[at, :] = mixed
            normed_ref[at, :] = rms_scale(mixed.astype(F32), gain_ref[...]).astype(BF16)
            return carry

        lax.fori_loop(0, half // CHUNK, finish, 0)

    out_buf[...] = (
        jnp.dot(placing, normed_ref[...], preferred_element_type=F32)
        .astype(BF16)
        .reshape(experts, cap, width)
    )

    upper = 2 * z // nz
    ahead = (z + nz - 1) // nz

    def order(j):
        return (j <= z) * (z - j) + (j > z) * j

    def turn(j):
        return order((j + ahead) % nz)

    def along(e):
        return remote(
            out_buf.at[e], arrived.at[z, t], a_send.at[e], a_recv.at[z], {"sp": 2 * e + c}
        )

    def along_in(p):
        return remote(
            arrived.at[p, t], arrived.at[p, t], a_send.at[p], a_recv.at[p], partner
        )

    def spread(p, k):
        block = arrived.at[p, t]
        return remote(
            block, block, b_send.at[k, p], b_recv.at[k, p], to_far if k else to_near
        )

    def spread_in(p, k):
        block = arrived.at[p, far_at if k else near_at]
        return remote(block, block, b_send.at[k, p], b_recv.at[k, p], partner)

    def forward(p):
        block = arrived.at[p, far_at]
        return remote(block, block, f_send.at[p], f_recv.at[p], to_near)

    def forward_in(p):
        block = arrived.at[p, flip(t, 3, n_tp)]
        return remote(block, block, f_send.at[p], f_recv.at[p], partner)

    def hand_over(p):
        return remote(
            part.at[p, flip(t, 3, n_tp)], hbuf.at[p], h_send.at[p], h_recv.at[p], to_near
        )

    def reduce_near(p):
        return remote(
            part.at[p, near_at], rbuf.at[p, 0], r_send.at[0, p], r_recv.at[0, p], to_near
        )

    def reduce_far(p):
        return remote(
            part.at[p, far_at], rbuf.at[p, 1], r_send.at[1, p], r_recv.at[1, p], to_far
        )

    def home(p):
        return remote(
            fin.at[p], ret.at[z], z_send.at[p], z_recv.at[z], {"sp": 2 * p + c}
        )

    def home_in(e):
        return remote(fin.at[e], ret.at[e], z_send.at[e], z_recv.at[e], partner)

    def launch(p):
        @pl.when(p != z)
        def _():
            along_in(p).wait_recv()

        spread(p, 0).start()
        spread(p, 1).start()

    arrived[z, t] = out_buf[z]

    def send_out(dz, carry):
        @pl.when(z - dz >= 0)
        def _():
            along(z - dz).start()

        @pl.when(z + dz < nz)
        def _():
            along(z + dz).start()

        return carry

    def pass_on(p):
        spread_in(p, 1).wait_recv()
        forward(p).start()

    send_out(1, 0)
    launch(order(0))

    @pl.when(ahead == 0)
    def _():
        pass_on(order(0))

    launch(order(1))
    lax.fori_loop(2, min(nz, 3), send_out, 0)

    @pl.when(ahead == 1)
    def _():
        pass_on(order(0))

    lax.fori_loop(3, nz, send_out, 0)

    @pl.when(ahead == 1)
    def _():
        pass_on(order(1))
        launch(order(2))

    for load in loads[1:]:
        load.wait()
    for swap in swaps:
        swap.wait_recv()

    def step(j, carry):
        @pl.when((j + 3 < nz) & (upper == 1))
        def _():
            launch(order(j + 3))

        @pl.when((j + 2 < nz) & (ahead == 1))
        def _():
            pass_on(order(j + 2))

        @pl.when(j < nz)
        def _():
            p = turn(j)
            spread_in(p, 0).wait_recv()
            forward_in(p).wait_recv()
            flat = arrived[p].reshape(n_tp * cap, width)
            result = None
            for i in range(2):
                gate = jnp.dot(flat, wg_ref[i], preferred_element_type=F32)
                up = jnp.dot(flat, wu_ref[i], preferred_element_type=F32)
                hidden = (gate * (1.0 / (1.0 + jnp.exp(-gate))) * up).astype(BF16)
                down = jnp.dot(hidden, wd_ref[i], preferred_element_type=F32)
                result = down if result is None else result + down
            part[p] = result.astype(BF16).reshape(n_tp, cap, width)
            hand_over(p).start()

            @pl.when((j < nz - 2) & (ahead == 1))
            def _():
                reduce_near(p).start()

        @pl.when((j + 1 < nz) & (ahead == 0))
        def _():
            pass_on(order(j + 1))

        @pl.when((j + 2 < nz) & (ahead == 0))
        def _():
            launch(order(j + 2))

        @pl.when((j >= 1) & (j <= nz))
        def _():
            p = turn(j - 1)
            hand_over(p).wait_recv()

            def one(r, carry):
                at = pl.ds(pl.multiple_of(r * CHUNK, CHUNK), CHUNK)
                total = part[p, far_at, at, :].astype(F32) + hbuf[p, at, :].astype(F32)
                part[p, far_at, at, :] = total.astype(BF16)
                return carry

            lax.fori_loop(0, cap // CHUNK, one, 0)
            reduce_far(p).start()

            @pl.when((j > nz - 2) | (ahead == 0))
            def _():
                reduce_near(p).start()

        @pl.when((j + 3 < nz) & (upper == 0) & (ahead == 1))
        def _():
            launch(order(j + 3))

        @pl.when((j >= 2) & (j - 2 < nz))
        def _():
            p = turn(j - 2)
            reduce_near(p).wait_recv()
            reduce_far(p).wait_recv()

            def one(r, carry):
                at = pl.ds(pl.multiple_of(r * CHUNK, CHUNK), CHUNK)
                total = (
                    part[p, t, at, :].astype(F32)
                    + rbuf[p, 0, at, :].astype(F32)
                    + rbuf[p, 1, at, :].astype(F32)
                )
                fin[p, at, :] = total.astype(BF16)
                return carry

            lax.fori_loop(0, cap // CHUNK, one, 0)

            @pl.when(p != z)
            def _():
                home(p).start()

            @pl.when(p == z)
            def _():
                ret[z] = fin[z]

        return carry

    lax.fori_loop(0, nz + 2, step, 0)

    def collect(dz, carry):
        home_in((z + dz) % nz).wait_recv()
        return carry

    lax.fori_loop(1, nz, collect, 0)

    both = jnp.concatenate(taking, axis=0)
    piece = width // 4
    for i in range(4):
        at = slice(i * piece, (i + 1) * piece)
        back = ret[:, :, at].reshape(n_slots, piece)
        rows_of = jnp.dot(both, back, preferred_element_type=F32)
        routed = weights[0] * rows_of[:share] + weights[1] * rows_of[share:]
        out_ref[:, at] = (mixed_ref[:, at].astype(F32) + routed).astype(BF16)

    def sent(dz, carry):
        p = (z + dz) % nz
        home(p).wait_send()
        along(p).wait_send()
        return carry

    lax.fori_loop(1, nz, sent, 0)

    def sent_plane(p, carry):
        for k in range(2):
            spread(p, k).wait_send()
        forward(p).wait_send()
        hand_over(p).wait_send()
        reduce_near(p).wait_send()
        reduce_far(p).wait_send()
        return carry

    lax.fori_loop(0, nz, sent_plane, 0)
    for i in range(2):
        ho_copy(i).wait_send()
        rn_copy(i).wait_send()
        rf_copy(i).wait_send()
    for swap in swaps:
        swap.wait_send()

    @pl.when(c == 0)
    def _():
        for copy in across(s, 0):
            copy.wait_send()

    @pl.when(z + 1 < nz)
    def _():
        for copy in chain(s, 0):
            copy.wait_send()

    def sent_source(dz, carry):
        source = 2 * (z - dz) + c
        for copy in across(source, dz):
            copy.wait_send()

        @pl.when(z + 1 < nz)
        def _():
            for copy in chain(source, dz):
                copy.wait_send()

        return carry

    lax.fori_loop(1, z + 1, sent_source, 0)


def local(
    nz,
    n_tp,
    queries,
    keys,
    values,
    log_gates,
    documents,
    query_gain,
    key_gain,
    out_weight,
    residual,
    norm_gain,
    routes,
    route_weights,
    w_gate,
    w_up,
    w_down,
):
    tok_dev, heads, hd = queries.shape
    rows_dev, width = residual.shape
    n_sp = 2 * nz
    named = min(rows_dev, 6 * rows_dev // n_sp)
    cap = named + (-named) % CHUNK
    hidden_dev = w_gate.shape[2]
    extra = LIMBS * heads + LIMBS + 1
    extra = extra + (-extra) % 16
    vmem = pl.BlockSpec(memory_space=pltpu.VMEM)
    hbm = pl.BlockSpec(memory_space=pl.ANY)
    dma = pltpu.SemaphoreType.DMA
    block = (cap, width)
    return pl.pallas_call(
        functools.partial(layer_kernel, nz, n_tp),
        out_shape=jax.ShapeDtypeStruct((rows_dev, width), BF16),
        in_specs=[vmem] * 7 + [hbm] + [vmem] * 4 + [hbm] * 3,
        out_specs=vmem,
        scratch_shapes=[
            pltpu.VMEM(out_weight.shape, BF16),
            pltpu.VMEM((2, width, hidden_dev), BF16),
            pltpu.VMEM((2, width, hidden_dev), BF16),
            pltpu.VMEM((2, hidden_dev, width), BF16),
            pltpu.VMEM((tok_dev * heads, hd), F32),
            pltpu.VMEM((heads, 2 * hd, tok_dev), BF16),
            pltpu.VMEM((extra, tok_dev), F32),
            pltpu.VMEM((hd, tok_dev), F32),
            pltpu.VMEM((n_sp, tok_dev, hd), BF16),
            pltpu.VMEM((n_sp, hd + extra, tok_dev), BF16),
            pltpu.VMEM((heads, 1, tok_dev), F32),
            pltpu.VMEM((heads, 1, tok_dev), F32),
            pltpu.VMEM((heads, hd, tok_dev), F32),
            pltpu.VMEM((tok_dev, heads * hd), BF16),
            pltpu.VMEM((n_tp, rows_dev, width), BF16),
            pltpu.VMEM((2, rows_dev // 2, width), BF16),
            pltpu.VMEM((2, rows_dev, width), BF16),
            pltpu.VMEM((rows_dev, width), BF16),
            pltpu.VMEM((rows_dev, width), BF16),
            pltpu.VMEM((nz,) + block, BF16),
            pltpu.VMEM((nz, n_tp) + block, BF16),
            pltpu.VMEM((nz, n_tp) + block, BF16),
            pltpu.VMEM((nz,) + block, BF16),
            pltpu.VMEM((nz, 2) + block, BF16),
            pltpu.VMEM((nz,) + block, BF16),
            pltpu.VMEM((nz,) + block, BF16),
            dma((4,)),
            dma((3,)),
            dma((3,)),
            dma((nz,)),
            dma((nz,)),
            dma((nz,)),
            dma((nz,)),
            dma((n_sp,)),
            dma((n_sp,)),
            dma((2,)),
            dma((2,)),
            dma((2,)),
            dma((2,)),
            dma((2,)),
            dma((2,)),
            dma((nz,)),
            dma((nz,)),
            dma((2, nz)),
            dma((2, nz)),
            dma((nz,)),
            dma((nz,)),
            dma((nz,)),
            dma((nz,)),
            dma((2, nz)),
            dma((2, nz)),
            dma((nz,)),
            dma((nz,)),
        ],
        compiler_params=pltpu.CompilerParams(
            collective_id=0, has_side_effects=True, vmem_limit_bytes=60 * 1024 * 1024
        ),
        name="layer",
    )(
        queries.reshape(tok_dev * heads, hd),
        keys.reshape(tok_dev, hd),
        values.reshape(tok_dev, hd),
        log_gates,
        documents[None, :],
        query_gain[None, :],
        key_gain[None, :],
        out_weight,
        residual,
        norm_gain[None, :],
        routes.T,
        route_weights.T,
        w_gate[0],
        w_up[0],
        w_down[0],
    )


def solution(mesh):
    return jax.shard_map(
        functools.partial(local, mesh.shape["sp"] // 2, mesh.shape["tp"]),
        mesh=mesh,
        in_specs=(
            P(("grp", "sp"), "tp", None),
            P(("grp", "sp"), "tp", None),
            P(("grp", "sp"), "tp", None),
            P("tp", ("grp", "sp")),
            P(("grp", "sp")),
            P(),
            P(),
            P("tp", None),
            P(("grp", "sp", "tp"), None),
            P(),
            P(("grp", "sp", "tp"), None),
            P(("grp", "sp", "tp"), None),
            P("sp", None, "tp"),
            P("sp", None, "tp"),
            P("sp", "tp", None),
        ),
        out_specs=P(("grp", "sp", "tp"), None),
        check_vma=False,
    )
```

```python
import functools

import jax
import jax.numpy as jnp
from jax import lax
from jax.experimental import pallas as pl
from jax.experimental.pallas import tpu as pltpu
from jax.sharding import PartitionSpec as P

EPSILON = 1e-06
CHUNK = 16
LIMBS = 3
MESH = pl.DeviceIdType.MESH
BF16 = jnp.bfloat16
F32 = jnp.float32


def rms_scale(inputs, gain):
    return inputs * lax.rsqrt(jnp.mean(inputs * inputs, axis=-1, keepdims=True) + EPSILON) * gain


def flip(index, bits, size):
    step = 1
    while step < size:
        bit = (bits // step) % 2
        index = index + bit * step * (1 - 2 * ((index // step) % 2))
        step *= 2
    return index


def remote(src, dst, send, recv, where):
    return pltpu.make_async_remote_copy(
        src, dst, send, recv, device_id=where, device_id_type=MESH
    )


KINDS = "LFCDRESN"
WORD = 10
PLANS = (
    ("SLFLSCFSLCFLDRFCDRCEDREDREE", "0123", "0123", "123", "123"),
    ("SLFLSCFSLCFLDRFCDRCEDREDREE", "0123", "0123", "123", "123"),
    ("SSLLFSFLFCRLFCRDCDECDREDREE", "1023", "0231", "023", "023"),
    ("SSLLFSFLFCRLFCRDCDECDREDREE", "1023", "0231", "023", "023"),
    ("SSSLLFFLLFCRFCRDCDECDREDREE", "2103", "1032", "310", "103"),
    ("SSSLLFFLLFCRFCRDCDECDREDREE", "2103", "1032", "310", "103"),
    ("SLLFSFSLLFCRFCRDCDECDREDREE", "3201", "2013", "201", "012"),
    ("SLLFSFSLLFCRFCRDCDECDREDREE", "3201", "2013", "201", "012"),
)


def plan(nz, s):
    if 2 * nz == len(PLANS):
        text, *lists = PLANS[s]
        return [text] + [[int(plane) for plane in planes] for planes in lists]
    z = s // 2
    text = "S" * (nz - 1) + "L" + "FL" * (nz - 1) + "F" + "CRD" * nz + "E" * nz
    planes = [(z + dz) % nz for dz in range(nz)]
    return [text, planes, planes[1:] + planes[:1], planes[1:], planes[1:]]


def packed(text):
    words = []
    for at in range(0, len(text), WORD):
        word = 0
        for kind in reversed(text[at:at + WORD]):
            word = word * len(KINDS) + KINDS.index(kind)
        words.append(word)
    return words


def chosen_by(index, values):
    total = 0
    for i, value in enumerate(values):
        total = total + (index == i) * value
    return total


def layer_kernel(
    nz,
    n_tp,
    q_ref,
    k_ref,
    v_ref,
    g_ref,
    d_ref,
    qg_ref,
    kg_ref,
    w_hbm,
    res_ref,
    gain_ref,
    rt_ref,
    rw_ref,
    wg_hbm,
    wu_hbm,
    wd_hbm,
    out_ref,
    w_ref,
    wg_ref,
    wu_ref,
    wd_ref,
    qf_ref,
    qt_ref,
    ext_ref,
    kx_ref,
    k_buf,
    v_buf,
    m_ref,
    l_ref,
    acc_ref,
    att_ref,
    sbuf,
    pho_buf,
    prs_buf,
    mixed_ref,
    normed_ref,
    out_buf,
    arrived,
    part,
    hbuf,
    rbuf,
    fin,
    ret,
    rout_ref,
    w_sem,
    wx_send,
    wx_recv,
    kc_send,
    vc_send,
    kx_send,
    vx_send,
    k_recv,
    v_recv,
    pho_send,
    pho_recv,
    prn_send,
    prn_recv,
    prf_send,
    prf_recv,
    a_send,
    a_recv,
    b_send,
    b_recv,
    f_send,
    f_recv,
    h_send,
    h_recv,
    r_send,
    r_recv,
    z_send,
    z_recv,
):
    s = lax.axis_index("sp")
    t = lax.axis_index("tp")
    z, c = s // 2, s % 2
    heads, rows, hd = acc_ref.shape[0], acc_ref.shape[2], acc_ref.shape[1]
    extra = ext_ref.shape[0]
    cap, width = out_buf.shape[1:]
    share = rows // n_tp
    half = share // 2
    partner = {"sp": 2 * z + 1 - c}
    near = 1 + c
    far = 2 - c
    near_at = flip(t, near, n_tp)
    far_at = flip(t, far, n_tp)
    to_near = {"tp": near_at}
    to_far = {"tp": far_at}

    barrier = pltpu.get_barrier_semaphore()
    for dz in range(1, nz):
        pl.semaphore_signal(
            barrier, inc=1, device_id={"sp": 2 * ((z + dz) % nz) + c}, device_id_type=MESH
        )
    for k in (1, 2):
        pl.semaphore_signal(
            barrier, inc=1, device_id={"tp": flip(t, k, n_tp)}, device_id_type=MESH
        )
    pl.semaphore_signal(barrier, inc=1, device_id=partner, device_id_type=MESH)
    loads = [
        pltpu.make_async_copy(src, dst, w_sem.at[i])
        for i, (src, dst) in enumerate(
            (
                (w_hbm, w_ref),
                (wg_hbm, wg_ref.at[0]),
                (wu_hbm, wu_ref.at[0]),
                (wd_hbm, wd_ref.at[0]),
            )
        )
    ]
    for load in loads:
        load.start()
    swaps = [
        remote(src, dst, wx_send.at[i], wx_recv.at[i], partner)
        for i, (src, dst) in enumerate(
            ((wg_hbm, wg_ref.at[1]), (wu_hbm, wu_ref.at[1]), (wd_hbm, wd_ref.at[1]))
        )
    ]

    k_buf[s] = rms_scale(k_ref[...].astype(F32), kg_ref[...]).astype(BF16)
    v_buf[s, 0:hd, :] = jnp.transpose(v_ref[...].astype(F32)).astype(BF16)
    gates = -g_ref[...]
    high = gates.astype(BF16).astype(F32)
    middle = (gates - high).astype(BF16).astype(F32)
    low = (gates - high - middle).astype(BF16).astype(F32)
    limbs = (high, middle, low)
    ext_ref[...] = jnp.zeros_like(ext_ref)
    for j, limb in enumerate(limbs):
        ext_ref[j * heads:(j + 1) * heads, :] = limb
    ones_at = LIMBS * heads
    doc_at = ones_at + LIMBS
    ext_ref[ones_at:ones_at + LIMBS, :] = jnp.ones((LIMBS, rows), F32)
    ext_ref[doc_at:doc_at + 1, :] = d_ref[...].astype(F32)
    v_buf[s, hd:hd + extra, :] = ext_ref[...].astype(BF16)

    pl.semaphore_wait(barrier, nz - 1 + 2 + 1)

    def chain(source, slot):
        there = {"sp": 2 * (z + 1) + c}
        return (
            remote(
                k_buf.at[source], k_buf.at[source], kc_send.at[slot], k_recv.at[source], there
            ),
            remote(
                v_buf.at[source], v_buf.at[source], vc_send.at[slot], v_recv.at[source], there
            ),
        )

    def across(source, slot):
        return (
            remote(
                k_buf.at[source], k_buf.at[source], kx_send.at[slot], k_recv.at[source], partner
            ),
            remote(
                v_buf.at[source], v_buf.at[source], vx_send.at[slot], v_recv.at[source], partner
            ),
        )

    @pl.when(z + 1 < nz)
    def _():
        for copy in chain(s, 0):
            copy.start()

    @pl.when(c == 0)
    def _():
        for copy in across(s, 0):
            copy.start()

    qf_ref[...] = q_ref[...].astype(F32)
    row = lax.broadcasted_iota(jnp.int32, (extra, rows), 0)
    for h in range(heads):
        picked = qf_ref[pl.ds(h, rows, stride=heads), :]
        query = (rms_scale(picked, qg_ref[...]) * hd ** (-0.5)).astype(BF16).astype(F32)
        lanes = slice(h * rows, (h + 1) * rows)
        qt_ref[0:hd, lanes] = jnp.transpose(query).astype(BF16)
        mine = jnp.where((row < ones_at) & (row % heads == h), 1.0, 0.0)
        for j, limb in enumerate(limbs):
            mine = jnp.where(row == ones_at + j, -limb[h:h + 1, :], mine)
        qt_ref[hd:hd + extra, lanes] = mine.astype(BF16)
        qt_ref[hd + extra:, lanes] = jnp.zeros((hd - extra, rows), BF16)
    kx_ref[...] = jnp.zeros_like(kx_ref)
    here = d_ref[...].astype(F32)

    def update(source, own):
        kx_ref[0:extra, :] = v_buf[source, hd:hd + extra, :].astype(F32)
        columns = jnp.transpose(kx_ref[...])
        left = jnp.concatenate([k_buf[source], columns.astype(BF16)], axis=1)
        same = columns[:, doc_at:doc_at + 1] == here
        if own:
            key_at = lax.broadcasted_iota(jnp.int32, (rows, rows), 0)
            query_at = lax.broadcasted_iota(jnp.int32, (rows, rows), 1)
            same = same & (key_at <= query_at)
        products = jnp.dot(left, qt_ref[...], preferred_element_type=F32)
        expos = []
        factors = []
        for h in range(heads):
            scores = jnp.where(same, products[:, h * rows:(h + 1) * rows], -jnp.inf)
            peak = jnp.max(scores, axis=0, keepdims=True)
            if own:
                new = peak
            else:
                old = m_ref[h]
                new = jnp.maximum(old, peak)
                factors.append(jnp.exp(old - new))
            expo = jnp.exp(scores - new)
            total = jnp.sum(expo, axis=0, keepdims=True)
            m_ref[h] = new
            l_ref[h] = total if own else factors[h] * l_ref[h] + total
            expos.append(expo.astype(BF16))
        mixes = jnp.dot(
            v_buf[source, 0:hd, :],
            jnp.concatenate(expos, axis=1),
            preferred_element_type=F32,
        )
        for h in range(heads):
            mix = mixes[:, h * rows:(h + 1) * rows]
            acc_ref[h] = mix if own else factors[h] * acc_ref[h] + mix

    update(s, True)

    def one_source(i, carry):
        dz = (i + 1) // 2
        direct = i % 2
        core = (1 - direct) * (1 - c) + direct * c
        source = 2 * (z - dz) + core
        onward = chain(source, dz)
        aside = across(source, dz)
        for k in range(2):
            aside[k].wait_recv()

            @pl.when(direct == 1)
            def _(k=k):
                @pl.when(z + 1 < nz)
                def _():
                    onward[k].start()

                aside[k].start()

        update(source, False)
        return carry

    lax.fori_loop(1 - c, 2 * z + 1, one_source, 0)

    for swap in swaps:
        swap.start()

    for h in range(heads):
        att_ref[:, h * hd:(h + 1) * hd] = jnp.transpose(acc_ref[h] * (1.0 / l_ref[h])).astype(BF16)

    def ho_copy(i):
        return remote(
            sbuf.at[3, pl.ds(i * half, half)], pho_buf.at[i], pho_send.at[i], pho_recv.at[i],
            to_near,
        )

    def rn_copy(i):
        return remote(
            sbuf.at[near, pl.ds(i * half, half)], prs_buf.at[0, pl.ds(i * half, half)],
            prn_send.at[i], prn_recv.at[i], to_near,
        )

    def rf_copy(i):
        return remote(
            sbuf.at[far, pl.ds(i * half, half)], prs_buf.at[1, pl.ds(i * half, half)],
            prf_send.at[i], prf_recv.at[i], to_far,
        )

    loads[0].wait()

    def project(k, column):
        start = pl.multiple_of(column * share, share)
        block = jnp.dot(
            att_ref[pl.ds(start, share), :], w_ref[...], preferred_element_type=F32
        )
        sbuf[k] = block.astype(BF16)

    def project_step(i, carry):
        k = (i == 0) * 3 + (i == 1) * near + (i == 2) * far
        project(k, flip(t, k, n_tp))

        @pl.when(i == 0)
        def _():
            for j in range(2):
                ho_copy(j).start()

        @pl.when(i == 1)
        def _():
            for j in range(2):
                rn_copy(j).start()

        return carry

    lax.fori_loop(0, n_tp, project_step, 0)

    for i in range(2):
        ho_copy(i).wait_recv()

        def pair(r, carry, i=i):
            at = pl.ds(pl.multiple_of(i * half + r * CHUNK, CHUNK), CHUNK)
            here_at = pl.ds(pl.multiple_of(r * CHUNK, CHUNK), CHUNK)
            total = sbuf[far, at, :].astype(F32) + pho_buf[i, here_at, :].astype(F32)
            sbuf[far, at, :] = total.astype(BF16)
            return carry

        lax.fori_loop(0, half // CHUNK, pair, 0)
        rf_copy(i).start()

    experts = nz
    padded = experts + (-experts) % 8
    n_slots = experts * cap
    first, second = rt_ref[0:1, :], rt_ref[1:2, :]
    names = lax.broadcasted_iota(jnp.int32, (padded, share), 0)
    chosen = [(names == first).astype(F32), (names == second).astype(F32)]
    up_to = lax.broadcasted_iota(jnp.int32, (share, share), 0) <= lax.broadcasted_iota(
        jnp.int32, (share, share), 1
    )
    rank = (
        jnp.dot(
            (chosen[0] + chosen[1]).astype(BF16),
            up_to.astype(F32).astype(BF16),
            preferred_element_type=F32,
        )
        - 1.0
    )
    start_of = names.astype(F32) * cap
    slots = [
        jnp.sum(choice * (rank + start_of), axis=0, keepdims=True) for choice in chosen
    ]
    slot_rows = lax.broadcasted_iota(jnp.int32, (n_slots, share), 0).astype(F32)
    placing = (
        (slot_rows == slots[0]).astype(F32) + (slot_rows == slots[1]).astype(F32)
    ).astype(BF16)
    diagonal = (
        lax.broadcasted_iota(jnp.int32, (share, share), 0)
        == lax.broadcasted_iota(jnp.int32, (share, share), 1)
    ).astype(F32)

    def column(values):
        return jnp.sum(diagonal * values, axis=1, keepdims=True)

    slot_of = jnp.concatenate([column(slot) for slot in slots], axis=0)
    weights = [column(rw_ref[k:k + 1, :]) for k in range(2)]

    for i in range(2):
        rn_copy(i).wait_recv()
        rf_copy(i).wait_recv()

        def finish(r, carry, i=i):
            at = pl.ds(pl.multiple_of(i * half + r * CHUNK, CHUNK), CHUNK)
            total = (
                sbuf[0, at, :].astype(F32)
                + prs_buf[0, at, :].astype(F32)
                + prs_buf[1, at, :].astype(F32)
            )
            mixed = (res_ref[at, :].astype(F32) + total).astype(BF16)
            mixed_ref[at, :] = mixed
            normed_ref[at, :] = rms_scale(mixed.astype(F32), gain_ref[...]).astype(BF16)
            return carry

        lax.fori_loop(0, half // CHUNK, finish, 0)

    out_buf[...] = (
        jnp.dot(placing, normed_ref[...], preferred_element_type=F32)
        .astype(BF16)
        .reshape(experts, cap, width)
    )

    plans = [plan(nz, i) for i in range(2 * nz)]
    longest = max(len(text) for text, *_ in plans)
    codes = [packed(text) for text, *_ in plans]
    codes = [
        chosen_by(s, [words[i] if i < len(words) else 0 for words in codes])
        for i in range(-(-longest // WORD))
    ]
    length = chosen_by(s, [len(text) for text, *_ in plans])
    orders, turns, targets, backs = (
        [chosen_by(s, planes) for planes in zip(*lists)]
        for lists in list(zip(*plans))[1:]
    )

    def order(j):
        return chosen_by(j, orders)

    def turn(j):
        return chosen_by(j, turns)

    def along(e):
        return remote(
            out_buf.at[e], arrived.at[z, t], a_send.at[e], a_recv.at[z], {"sp": 2 * e + c}
        )

    def along_in(p):
        return remote(
            arrived.at[p, t], arrived.at[p, t], a_send.at[p], a_recv.at[p], partner
        )

    def spread(p, k):
        block = arrived.at[p, t]
        return remote(
            block, block, b_send.at[k, p], b_recv.at[k, p], to_far if k else to_near
        )

    def spread_in(p, k):
        block = arrived.at[p, far_at if k else near_at]
        return remote(block, block, b_send.at[k, p], b_recv.at[k, p], partner)

    def forward(p):
        block = arrived.at[p, far_at]
        return remote(block, block, f_send.at[p], f_recv.at[p], to_near)

    def forward_in(p):
        block = arrived.at[p, flip(t, 3, n_tp)]
        return remote(block, block, f_send.at[p], f_recv.at[p], partner)

    def hand_over(p):
        return remote(
            part.at[p, flip(t, 3, n_tp)], hbuf.at[p], h_send.at[p], h_recv.at[p], to_near
        )

    def reduce_near(p):
        return remote(
            part.at[p, near_at], rbuf.at[p, 0], r_send.at[0, p], r_recv.at[0, p], to_near
        )

    def reduce_far(p):
        return remote(
            part.at[p, far_at], rbuf.at[p, 1], r_send.at[1, p], r_recv.at[1, p], to_far
        )

    def home(p):
        return remote(
            fin.at[p], ret.at[z], z_send.at[p], z_recv.at[z], {"sp": 2 * p + c}
        )

    def home_in(e):
        return remote(fin.at[e], ret.at[e], z_send.at[e], z_recv.at[e], partner)

    def launch(p):
        @pl.when(p != z)
        def _():
            along_in(p).wait_recv()

        spread(p, 0).start()
        spread(p, 1).start()

    arrived[z, t] = out_buf[z]

    def pass_on(p):
        spread_in(p, 1).wait_recv()
        forward(p).start()

    for load in loads[1:]:
        load.wait()

    def compute(p, index):
        @pl.when(index == 0)
        def _():
            for swap in swaps:
                swap.wait_recv()

        spread_in(p, 0).wait_recv()
        forward_in(p).wait_recv()
        flat = arrived[p].reshape(n_tp * cap, width)
        result = None
        for i in range(2):
            gate = jnp.dot(flat, wg_ref[i], preferred_element_type=F32)
            up = jnp.dot(flat, wu_ref[i], preferred_element_type=F32)
            hidden = (gate * (1.0 / (1.0 + jnp.exp(-gate))) * up).astype(BF16)
            down = jnp.dot(hidden, wd_ref[i], preferred_element_type=F32)
            result = down if result is None else result + down
        part[p] = result.astype(BF16).reshape(n_tp, cap, width)
        hand_over(p).start()

    def add_far(p):
        hand_over(p).wait_recv()

        def one(r, carry):
            at = pl.ds(pl.multiple_of(r * CHUNK, CHUNK), CHUNK)
            total = part[p, far_at, at, :].astype(F32) + hbuf[p, at, :].astype(F32)
            part[p, far_at, at, :] = total.astype(BF16)
            return carry

        lax.fori_loop(0, cap // CHUNK, one, 0)
        reduce_far(p).start()

    def end(p):
        reduce_near(p).wait_recv()
        reduce_far(p).wait_recv()

        def one(r, carry):
            at = pl.ds(pl.multiple_of(r * CHUNK, CHUNK), CHUNK)
            total = (
                part[p, t, at, :].astype(F32)
                + rbuf[p, 0, at, :].astype(F32)
                + rbuf[p, 1, at, :].astype(F32)
            )
            fin[p, at, :] = total.astype(BF16)
            return carry

        lax.fori_loop(0, cap // CHUNK, one, 0)

        @pl.when(p != z)
        def _():
            home(p).start()

        @pl.when(p == z)
        def _():
            ret[z] = fin[z]

    doing = {
        "L": lambda j: launch(order(j)),
        "F": lambda j: pass_on(order(j)),
        "C": lambda j: compute(turn(j), j),
        "D": lambda j: add_far(turn(j)),
        "R": lambda j: reduce_near(turn(j)).start(),
        "E": lambda j: end(turn(j)),
        "S": lambda j: along(chosen_by(j, targets)).start(),
    }

    def tick(i, carry):
        code, counts = carry
        fresh = (i % WORD) == 0
        code = jnp.where(fresh, chosen_by(i // WORD, codes), code // len(KINDS))
        kind = code % len(KINDS)
        for k, name in enumerate(KINDS[:len(doing)]):
            @pl.when(kind == k)
            def _(k=k, name=name):
                doing[name](counts[k])

        counts = tuple(count + (kind == k) for k, count in enumerate(counts))
        return code, counts

    zero = jnp.int32(0)
    lax.fori_loop(0, length, tick, (zero, (zero,) * len(KINDS)))

    numbers = lax.broadcasted_iota(jnp.int32, (2 * share, cap), 1).astype(F32)
    piece = width // 4

    def gather(e, finish):
        taking = (numbers + (e * cap).astype(F32) == slot_of).astype(F32).astype(BF16)
        for i in range(4):
            at = slice(i * piece, (i + 1) * piece)
            found = jnp.dot(taking, ret[e, :, at], preferred_element_type=F32)
            routed = rout_ref[:, at] + weights[0] * found[:share] + weights[1] * found[share:]
            if finish:
                out_ref[:, at] = (mixed_ref[:, at].astype(F32) + routed).astype(BF16)
            else:
                rout_ref[:, at] = routed

    rout_ref[...] = jnp.zeros_like(rout_ref)
    gather(z, False)

    def collect(i, carry):
        e = chosen_by(i, backs)
        home_in(e).wait_recv()
        gather(e, False)
        return carry

    lax.fori_loop(0, nz - 2, collect, 0)
    final = backs[nz - 2]
    home_in(final).wait_recv()
    gather(final, True)

    def sent(dz, carry):
        p = (z + dz) % nz
        home(p).wait_send()
        along(p).wait_send()
        return carry

    lax.fori_loop(1, nz, sent, 0)

    def sent_plane(p, carry):
        for k in range(2):
            spread(p, k).wait_send()
        forward(p).wait_send()
        hand_over(p).wait_send()
        reduce_near(p).wait_send()
        reduce_far(p).wait_send()
        return carry

    lax.fori_loop(0, nz, sent_plane, 0)
    for i in range(2):
        ho_copy(i).wait_send()
        rn_copy(i).wait_send()
        rf_copy(i).wait_send()
    for swap in swaps:
        swap.wait_send()

    @pl.when(c == 0)
    def _():
        for copy in across(s, 0):
            copy.wait_send()

    @pl.when(z + 1 < nz)
    def _():
        for copy in chain(s, 0):
            copy.wait_send()

    def sent_source(dz, carry):
        source = 2 * (z - dz) + c
        for copy in across(source, dz):
            copy.wait_send()

        @pl.when(z + 1 < nz)
        def _():
            for copy in chain(source, dz):
                copy.wait_send()

        return carry

    lax.fori_loop(1, z + 1, sent_source, 0)


def local(
    nz,
    n_tp,
    queries,
    keys,
    values,
    log_gates,
    documents,
    query_gain,
    key_gain,
    out_weight,
    residual,
    norm_gain,
    routes,
    route_weights,
    w_gate,
    w_up,
    w_down,
):
    tok_dev, heads, hd = queries.shape
    rows_dev, width = residual.shape
    n_sp = 2 * nz
    named = min(rows_dev, 6 * rows_dev // n_sp)
    cap = named + (-named) % CHUNK
    hidden_dev = w_gate.shape[2]
    extra = LIMBS * heads + LIMBS + 1
    extra = extra + (-extra) % 16
    vmem = pl.BlockSpec(memory_space=pltpu.VMEM)
    hbm = pl.BlockSpec(memory_space=pl.ANY)
    dma = pltpu.SemaphoreType.DMA
    block = (cap, width)
    return pl.pallas_call(
        functools.partial(layer_kernel, nz, n_tp),
        out_shape=jax.ShapeDtypeStruct((rows_dev, width), BF16),
        in_specs=[vmem] * 7 + [hbm] + [vmem] * 4 + [hbm] * 3,
        out_specs=vmem,
        scratch_shapes=[
            pltpu.VMEM(out_weight.shape, BF16),
            pltpu.VMEM((2, width, hidden_dev), BF16),
            pltpu.VMEM((2, width, hidden_dev), BF16),
            pltpu.VMEM((2, hidden_dev, width), BF16),
            pltpu.VMEM((tok_dev * heads, hd), F32),
            pltpu.VMEM((2 * hd, heads * tok_dev), BF16),
            pltpu.VMEM((extra, tok_dev), F32),
            pltpu.VMEM((hd, tok_dev), F32),
            pltpu.VMEM((n_sp, tok_dev, hd), BF16),
            pltpu.VMEM((n_sp, hd + extra, tok_dev), BF16),
            pltpu.VMEM((heads, 1, tok_dev), F32),
            pltpu.VMEM((heads, 1, tok_dev), F32),
            pltpu.VMEM((heads, hd, tok_dev), F32),
            pltpu.VMEM((tok_dev, heads * hd), BF16),
            pltpu.VMEM((n_tp, rows_dev, width), BF16),
            pltpu.VMEM((2, rows_dev // 2, width), BF16),
            pltpu.VMEM((2, rows_dev, width), BF16),
            pltpu.VMEM((rows_dev, width), BF16),
            pltpu.VMEM((rows_dev, width), BF16),
            pltpu.VMEM((nz,) + block, BF16),
            pltpu.VMEM((nz, n_tp) + block, BF16),
            pltpu.VMEM((nz, n_tp) + block, BF16),
            pltpu.VMEM((nz,) + block, BF16),
            pltpu.VMEM((nz, 2) + block, BF16),
            pltpu.VMEM((nz,) + block, BF16),
            pltpu.VMEM((nz,) + block, BF16),
            pltpu.VMEM((rows_dev, width), F32),
            dma((4,)),
            dma((3,)),
            dma((3,)),
            dma((nz,)),
            dma((nz,)),
            dma((nz,)),
            dma((nz,)),
            dma((n_sp,)),
            dma((n_sp,)),
            dma((2,)),
            dma((2,)),
            dma((2,)),
            dma((2,)),
            dma((2,)),
            dma((2,)),
            dma((nz,)),
            dma((nz,)),
            dma((2, nz)),
            dma((2, nz)),
            dma((nz,)),
            dma((nz,)),
            dma((nz,)),
            dma((nz,)),
            dma((2, nz)),
            dma((2, nz)),
            dma((nz,)),
            dma((nz,)),
        ],
        compiler_params=pltpu.CompilerParams(
            collective_id=0, has_side_effects=True, vmem_limit_bytes=60 * 1024 * 1024
        ),
        name="layer",
    )(
        queries.reshape(tok_dev * heads, hd),
        keys.reshape(tok_dev, hd),
        values.reshape(tok_dev, hd),
        log_gates,
        documents[None, :],
        query_gain[None, :],
        key_gain[None, :],
        out_weight,
        residual,
        norm_gain[None, :],
        routes.T,
        route_weights.T,
        w_gate[0],
        w_up[0],
        w_down[0],
    )


def solution(mesh):
    return jax.shard_map(
        functools.partial(local, mesh.shape["sp"] // 2, mesh.shape["tp"]),
        mesh=mesh,
        in_specs=(
            P(("grp", "sp"), "tp", None),
            P(("grp", "sp"), "tp", None),
            P(("grp", "sp"), "tp", None),
            P("tp", ("grp", "sp")),
            P(("grp", "sp")),
            P(),
            P(),
            P("tp", None),
            P(("grp", "sp", "tp"), None),
            P(),
            P(("grp", "sp", "tp"), None),
            P(("grp", "sp", "tp"), None),
            P("sp", None, "tp"),
            P("sp", None, "tp"),
            P("sp", "tp", None),
        ),
        out_specs=P(("grp", "sp", "tp"), None),
        check_vma=False,
    )
```

```python
import functools

import jax
import jax.numpy as jnp
from jax import lax
from jax.experimental import pallas as pl
from jax.experimental.pallas import tpu as pltpu
from jax.sharding import PartitionSpec as P

EPSILON = 1e-06
CHUNK = 16
LIMBS = 3
MESH = pl.DeviceIdType.MESH
BF16 = jnp.bfloat16
F32 = jnp.float32


def rms_scale(inputs, gain):
    return inputs * lax.rsqrt(jnp.mean(inputs * inputs, axis=-1, keepdims=True) + EPSILON) * gain


def flip(index, bits, size):
    step = 1
    while step < size:
        bit = (bits // step) % 2
        index = index + bit * step * (1 - 2 * ((index // step) % 2))
        step *= 2
    return index


def remote(src, dst, send, recv, where):
    return pltpu.make_async_remote_copy(
        src, dst, send, recv, device_id=where, device_id_type=MESH
    )


KINDS = "LFCDRESN"
WORD = 10
PLANS = (
    ("SLFLSCFSLCFLDRFCDRCEDREDREE", "0123", "0123", "123", "123"),
    ("SLFLSCFSLCFLDRFCDRCEDREDREE", "0123", "0123", "123", "123"),
    ("SSLLFSFLFCRLFCRDCDEDRECEDRE", "1023", "0231", "023", "023"),
    ("SSLLFSFLFCRLFCRDCDEDRECEDRE", "1023", "0231", "023", "023"),
    ("SSSLLFFLLFCRFCRDCDEDRECEDRE", "2103", "1032", "310", "103"),
    ("SSSLLFFLLFCRFCRDCDEDRECEDRE", "2103", "1032", "310", "103"),
    ("SLLFSFSLLFCRFCRDCDECDREDREE", "3201", "2013", "201", "012"),
    ("SLLFSFSLLFCRFCRDCDECDREDREE", "3201", "2013", "201", "012"),
)


def plan(nz, s):
    if 2 * nz == len(PLANS):
        text, *lists = PLANS[s]
        return [text] + [[int(plane) for plane in planes] for planes in lists]
    z = s // 2
    text = "S" * (nz - 1) + "L" + "FL" * (nz - 1) + "F" + "CRD" * nz + "E" * nz
    planes = [(z + dz) % nz for dz in range(nz)]
    return [text, planes, planes[1:] + planes[:1], planes[1:], planes[1:]]


def packed(text):
    words = []
    for at in range(0, len(text), WORD):
        word = 0
        for kind in reversed(text[at:at + WORD]):
            word = word * len(KINDS) + KINDS.index(kind)
        words.append(word)
    return words


def chosen_by(index, values):
    total = 0
    for i, value in enumerate(values):
        total = total + (index == i) * value
    return total


def entry(nz, n_tp, *refs):
    small = refs[:7] + refs[8:12]
    held = refs[16:16 + len(small)]
    fills = [
        pltpu.make_async_copy(src, dst, refs[-1].at[i])
        for i, (src, dst) in enumerate(zip(small, held))
    ]
    layer_kernel(
        nz, n_tp, fills, *held[:7], refs[7], *held[7:], *refs[12:16],
        *refs[16 + len(small):-1],
    )


def layer_kernel(
    nz,
    n_tp,
    fills,
    q_ref,
    k_ref,
    v_ref,
    g_ref,
    d_ref,
    qg_ref,
    kg_ref,
    w_hbm,
    res_ref,
    gain_ref,
    rt_ref,
    rw_ref,
    wg_hbm,
    wu_hbm,
    wd_hbm,
    out_ref,
    w_ref,
    wg_ref,
    wu_ref,
    wd_ref,
    qf_ref,
    qt_ref,
    ext_ref,
    kx_ref,
    k_buf,
    v_buf,
    m_ref,
    l_ref,
    acc_ref,
    att_ref,
    sbuf,
    pho_buf,
    prs_buf,
    mixed_ref,
    normed_ref,
    out_buf,
    arrived,
    part,
    hbuf,
    rbuf,
    fin,
    ret,
    rout_ref,
    w_sem,
    wx_send,
    wx_recv,
    kc_send,
    vc_send,
    kx_send,
    vx_send,
    k_recv,
    v_recv,
    pho_send,
    pho_recv,
    prn_send,
    prn_recv,
    prf_send,
    prf_recv,
    a_send,
    a_recv,
    b_send,
    b_recv,
    f_send,
    f_recv,
    h_send,
    h_recv,
    r_send,
    r_recv,
    z_send,
    z_recv,
):
    s = lax.axis_index("sp")
    t = lax.axis_index("tp")
    z, c = s // 2, s % 2
    heads, rows, hd = acc_ref.shape[0], acc_ref.shape[2], acc_ref.shape[1]
    extra = ext_ref.shape[0]
    cap, width = out_buf.shape[1:]
    share = rows // n_tp
    half = share // 2
    partner = {"sp": 2 * z + 1 - c}
    near = 1 + c
    far = 2 - c
    near_at = flip(t, near, n_tp)
    far_at = flip(t, far, n_tp)
    to_near = {"tp": near_at}
    to_far = {"tp": far_at}

    barrier = pltpu.get_barrier_semaphore()
    for dz in range(1, nz):
        pl.semaphore_signal(
            barrier, inc=1, device_id={"sp": 2 * ((z + dz) % nz) + c}, device_id_type=MESH
        )
    for k in (1, 2):
        pl.semaphore_signal(
            barrier, inc=1, device_id={"tp": flip(t, k, n_tp)}, device_id_type=MESH
        )
    pl.semaphore_signal(barrier, inc=1, device_id=partner, device_id_type=MESH)
    loads = [
        pltpu.make_async_copy(src, dst, w_sem.at[i])
        for i, (src, dst) in enumerate(
            (
                (w_hbm, w_ref),
                (wg_hbm, wg_ref.at[0]),
                (wu_hbm, wu_ref.at[0]),
                (wd_hbm, wd_ref.at[0]),
            )
        )
    ]
    first = (1, 2, 3, 4, 6)
    for i in first:
        fills[i].start()
    for i, fill in enumerate(fills):
        if i not in first:
            fill.start()
    swaps = [
        remote(src, dst, wx_send.at[i], wx_recv.at[i], partner)
        for i, (src, dst) in enumerate(
            ((wg_hbm, wg_ref.at[1]), (wu_hbm, wu_ref.at[1]), (wd_hbm, wd_ref.at[1]))
        )
    ]

    for i in first:
        fills[i].wait()
    k_buf[s] = rms_scale(k_ref[...].astype(F32), kg_ref[...]).astype(BF16)
    v_buf[s, 0:hd, :] = jnp.transpose(v_ref[...].astype(F32)).astype(BF16)
    gates = -g_ref[...]
    high = gates.astype(BF16).astype(F32)
    middle = (gates - high).astype(BF16).astype(F32)
    low = (gates - high - middle).astype(BF16).astype(F32)
    limbs = (high, middle, low)
    ext_ref[...] = jnp.zeros_like(ext_ref)
    for j, limb in enumerate(limbs):
        ext_ref[j * heads:(j + 1) * heads, :] = limb
    ones_at = LIMBS * heads
    doc_at = ones_at + LIMBS
    ext_ref[ones_at:ones_at + LIMBS, :] = jnp.ones((LIMBS, rows), F32)
    ext_ref[doc_at:doc_at + 1, :] = d_ref[...].astype(F32)
    v_buf[s, hd:hd + extra, :] = ext_ref[...].astype(BF16)

    pl.semaphore_wait(barrier, nz - 1 + 2 + 1)

    def chain(source, slot):
        there = {"sp": 2 * (z + 1) + c}
        return (
            remote(
                k_buf.at[source], k_buf.at[source], kc_send.at[slot], k_recv.at[source], there
            ),
            remote(
                v_buf.at[source], v_buf.at[source], vc_send.at[slot], v_recv.at[source], there
            ),
        )

    def across(source, slot):
        return (
            remote(
                k_buf.at[source], k_buf.at[source], kx_send.at[slot], k_recv.at[source], partner
            ),
            remote(
                v_buf.at[source], v_buf.at[source], vx_send.at[slot], v_recv.at[source], partner
            ),
        )

    @pl.when(z + 1 < nz)
    def _():
        for copy in chain(s, 0):
            copy.start()

    @pl.when(c == 0)
    def _():
        for copy in across(s, 0):
            copy.start()

    for i, fill in enumerate(fills):
        if i not in first:
            fill.wait()
    for load in loads:
        load.start()

    qf_ref[...] = q_ref[...].astype(F32)
    row = lax.broadcasted_iota(jnp.int32, (extra, rows), 0)
    for h in range(heads):
        picked = qf_ref[pl.ds(h, rows, stride=heads), :]
        query = (rms_scale(picked, qg_ref[...]) * hd ** (-0.5)).astype(BF16).astype(F32)
        lanes = slice(h * rows, (h + 1) * rows)
        qt_ref[0:hd, lanes] = jnp.transpose(query).astype(BF16)
        mine = jnp.where((row < ones_at) & (row % heads == h), 1.0, 0.0)
        for j, limb in enumerate(limbs):
            mine = jnp.where(row == ones_at + j, -limb[h:h + 1, :], mine)
        qt_ref[hd:hd + extra, lanes] = mine.astype(BF16)
        qt_ref[hd + extra:, lanes] = jnp.zeros((hd - extra, rows), BF16)
    kx_ref[...] = jnp.zeros_like(kx_ref)
    here = d_ref[...].astype(F32)

    def update(source, own):
        kx_ref[0:extra, :] = v_buf[source, hd:hd + extra, :].astype(F32)
        columns = jnp.transpose(kx_ref[...])
        left = jnp.concatenate([k_buf[source], columns.astype(BF16)], axis=1)
        same = columns[:, doc_at:doc_at + 1] == here
        if own:
            key_at = lax.broadcasted_iota(jnp.int32, (rows, rows), 0)
            query_at = lax.broadcasted_iota(jnp.int32, (rows, rows), 1)
            same = same & (key_at <= query_at)
        products = jnp.dot(left, qt_ref[...], preferred_element_type=F32)
        expos = []
        factors = []
        for h in range(heads):
            scores = jnp.where(same, products[:, h * rows:(h + 1) * rows], -jnp.inf)
            peak = jnp.max(scores, axis=0, keepdims=True)
            if own:
                new = peak
            else:
                old = m_ref[h]
                new = jnp.maximum(old, peak)
                factors.append(jnp.exp(old - new))
            expo = jnp.exp(scores - new)
            total = jnp.sum(expo, axis=0, keepdims=True)
            m_ref[h] = new
            l_ref[h] = total if own else factors[h] * l_ref[h] + total
            expos.append(expo.astype(BF16))
        mixes = jnp.dot(
            v_buf[source, 0:hd, :],
            jnp.concatenate(expos, axis=1),
            preferred_element_type=F32,
        )
        for h in range(heads):
            mix = mixes[:, h * rows:(h + 1) * rows]
            acc_ref[h] = mix if own else factors[h] * acc_ref[h] + mix

    update(s, True)

    def one_source(i, carry):
        dz = (i + 1) // 2
        direct = i % 2
        core = (1 - direct) * (1 - c) + direct * c
        source = 2 * (z - dz) + core
        onward = chain(source, dz)
        aside = across(source, dz)
        for k in range(2):
            aside[k].wait_recv()

            @pl.when(direct == 1)
            def _(k=k):
                @pl.when(z + 1 < nz)
                def _():
                    onward[k].start()

                aside[k].start()

        update(source, False)
        return carry

    lax.fori_loop(1 - c, 2 * z + 1, one_source, 0)

    for swap in swaps:
        swap.start()

    for h in range(heads):
        att_ref[:, h * hd:(h + 1) * hd] = jnp.transpose(acc_ref[h] * (1.0 / l_ref[h])).astype(BF16)

    def ho_copy(i):
        return remote(
            sbuf.at[3, pl.ds(i * half, half)], pho_buf.at[i], pho_send.at[i], pho_recv.at[i],
            to_near,
        )

    def rn_copy(i):
        return remote(
            sbuf.at[near, pl.ds(i * half, half)], prs_buf.at[0, pl.ds(i * half, half)],
            prn_send.at[i], prn_recv.at[i], to_near,
        )

    def rf_copy(i):
        return remote(
            sbuf.at[far, pl.ds(i * half, half)], prs_buf.at[1, pl.ds(i * half, half)],
            prf_send.at[i], prf_recv.at[i], to_far,
        )

    loads[0].wait()

    def project(k, column):
        start = pl.multiple_of(column * share, share)
        block = jnp.dot(
            att_ref[pl.ds(start, share), :], w_ref[...], preferred_element_type=F32
        )
        sbuf[k] = block.astype(BF16)

    def project_step(i, carry):
        k = (i == 0) * 3 + (i == 1) * near + (i == 2) * far
        project(k, flip(t, k, n_tp))

        @pl.when(i == 0)
        def _():
            for j in range(2):
                ho_copy(j).start()

        @pl.when(i == 1)
        def _():
            for j in range(2):
                rn_copy(j).start()

        return carry

    lax.fori_loop(0, n_tp, project_step, 0)

    for i in range(2):
        ho_copy(i).wait_recv()

        def pair(r, carry, i=i):
            at = pl.ds(pl.multiple_of(i * half + r * CHUNK, CHUNK), CHUNK)
            here_at = pl.ds(pl.multiple_of(r * CHUNK, CHUNK), CHUNK)
            total = sbuf[far, at, :].astype(F32) + pho_buf[i, here_at, :].astype(F32)
            sbuf[far, at, :] = total.astype(BF16)
            return carry

        lax.fori_loop(0, half // CHUNK, pair, 0)
        rf_copy(i).start()

    experts = nz
    padded = experts + (-experts) % 8
    n_slots = experts * cap
    first, second = rt_ref[0:1, :], rt_ref[1:2, :]
    names = lax.broadcasted_iota(jnp.int32, (padded, share), 0)
    chosen = [(names == first).astype(F32), (names == second).astype(F32)]
    up_to = lax.broadcasted_iota(jnp.int32, (share, share), 0) <= lax.broadcasted_iota(
        jnp.int32, (share, share), 1
    )
    rank = (
        jnp.dot(
            (chosen[0] + chosen[1]).astype(BF16),
            up_to.astype(F32).astype(BF16),
            preferred_element_type=F32,
        )
        - 1.0
    )
    start_of = names.astype(F32) * cap
    slots = [
        jnp.sum(choice * (rank + start_of), axis=0, keepdims=True) for choice in chosen
    ]
    slot_rows = lax.broadcasted_iota(jnp.int32, (n_slots, share), 0).astype(F32)
    placing = (
        (slot_rows == slots[0]).astype(F32) + (slot_rows == slots[1]).astype(F32)
    ).astype(BF16)
    diagonal = (
        lax.broadcasted_iota(jnp.int32, (share, share), 0)
        == lax.broadcasted_iota(jnp.int32, (share, share), 1)
    ).astype(F32)

    def column(values):
        return jnp.sum(diagonal * values, axis=1, keepdims=True)

    slot_of = jnp.concatenate([column(slot) for slot in slots], axis=0)
    weights = [column(rw_ref[k:k + 1, :]) for k in range(2)]

    for i in range(2):
        rn_copy(i).wait_recv()
        rf_copy(i).wait_recv()

        def finish(r, carry, i=i):
            at = pl.ds(pl.multiple_of(i * half + r * CHUNK, CHUNK), CHUNK)
            total = (
                sbuf[0, at, :].astype(F32)
                + prs_buf[0, at, :].astype(F32)
                + prs_buf[1, at, :].astype(F32)
            )
            mixed = (res_ref[at, :].astype(F32) + total).astype(BF16)
            mixed_ref[at, :] = mixed
            normed_ref[at, :] = rms_scale(mixed.astype(F32), gain_ref[...]).astype(BF16)
            return carry

        lax.fori_loop(0, half // CHUNK, finish, 0)

    out_buf[...] = (
        jnp.dot(placing, normed_ref[...], preferred_element_type=F32)
        .astype(BF16)
        .reshape(experts, cap, width)
    )

    plans = [plan(nz, i) for i in range(2 * nz)]
    longest = max(len(text) for text, *_ in plans)
    codes = [packed(text) for text, *_ in plans]
    codes = [
        chosen_by(s, [words[i] if i < len(words) else 0 for words in codes])
        for i in range(-(-longest // WORD))
    ]
    length = chosen_by(s, [len(text) for text, *_ in plans])
    orders, turns, targets, backs = (
        [chosen_by(s, planes) for planes in zip(*lists)]
        for lists in list(zip(*plans))[1:]
    )

    def order(j):
        return chosen_by(j, orders)

    def turn(j):
        return chosen_by(j, turns)

    def along(e):
        return remote(
            out_buf.at[e], arrived.at[z, t], a_send.at[e], a_recv.at[z], {"sp": 2 * e + c}
        )

    def along_in(p):
        return remote(
            arrived.at[p, t], arrived.at[p, t], a_send.at[p], a_recv.at[p], partner
        )

    def spread(p, k):
        block = arrived.at[p, t]
        return remote(
            block, block, b_send.at[k, p], b_recv.at[k, p], to_far if k else to_near
        )

    def spread_in(p, k):
        block = arrived.at[p, far_at if k else near_at]
        return remote(block, block, b_send.at[k, p], b_recv.at[k, p], partner)

    def forward(p):
        block = arrived.at[p, far_at]
        return remote(block, block, f_send.at[p], f_recv.at[p], to_near)

    def forward_in(p):
        block = arrived.at[p, flip(t, 3, n_tp)]
        return remote(block, block, f_send.at[p], f_recv.at[p], partner)

    def hand_over(p):
        return remote(
            part.at[p, flip(t, 3, n_tp)], hbuf.at[p], h_send.at[p], h_recv.at[p], to_near
        )

    def reduce_near(p):
        return remote(
            part.at[p, near_at], rbuf.at[p, 0], r_send.at[0, p], r_recv.at[0, p], to_near
        )

    def reduce_far(p):
        return remote(
            part.at[p, far_at], rbuf.at[p, 1], r_send.at[1, p], r_recv.at[1, p], to_far
        )

    def home(p):
        return remote(
            fin.at[p], ret.at[z], z_send.at[p], z_recv.at[z], {"sp": 2 * p + c}
        )

    def home_in(e):
        return remote(fin.at[e], ret.at[e], z_send.at[e], z_recv.at[e], partner)

    def launch(p):
        @pl.when(p != z)
        def _():
            along_in(p).wait_recv()

        spread(p, 0).start()
        spread(p, 1).start()

    arrived[z, t] = out_buf[z]

    def pass_on(p):
        spread_in(p, 1).wait_recv()
        forward(p).start()

    for load in loads[1:]:
        load.wait()

    def compute(p, index):
        @pl.when(index == 0)
        def _():
            for swap in swaps:
                swap.wait_recv()

        spread_in(p, 0).wait_recv()
        forward_in(p).wait_recv()
        flat = arrived[p].reshape(n_tp * cap, width)
        result = None
        for i in range(2):
            gate = jnp.dot(flat, wg_ref[i], preferred_element_type=F32)
            up = jnp.dot(flat, wu_ref[i], preferred_element_type=F32)
            hidden = (gate * (1.0 / (1.0 + jnp.exp(-gate))) * up).astype(BF16)
            down = jnp.dot(hidden, wd_ref[i], preferred_element_type=F32)
            result = down if result is None else result + down
        part[p] = result.astype(BF16).reshape(n_tp, cap, width)
        hand_over(p).start()

    def add_far(p):
        hand_over(p).wait_recv()

        def one(r, carry):
            at = pl.ds(pl.multiple_of(r * CHUNK, CHUNK), CHUNK)
            total = part[p, far_at, at, :].astype(F32) + hbuf[p, at, :].astype(F32)
            part[p, far_at, at, :] = total.astype(BF16)
            return carry

        lax.fori_loop(0, cap // CHUNK, one, 0)
        reduce_far(p).start()

    def end(p):
        reduce_near(p).wait_recv()
        reduce_far(p).wait_recv()

        def one(r, carry):
            at = pl.ds(pl.multiple_of(r * CHUNK, CHUNK), CHUNK)
            total = (
                part[p, t, at, :].astype(F32)
                + rbuf[p, 0, at, :].astype(F32)
                + rbuf[p, 1, at, :].astype(F32)
            )
            fin[p, at, :] = total.astype(BF16)
            return carry

        lax.fori_loop(0, cap // CHUNK, one, 0)

        @pl.when(p != z)
        def _():
            home(p).start()

        @pl.when(p == z)
        def _():
            ret[z] = fin[z]

    doing = {
        "L": lambda j: launch(order(j)),
        "F": lambda j: pass_on(order(j)),
        "C": lambda j: compute(turn(j), j),
        "D": lambda j: add_far(turn(j)),
        "R": lambda j: reduce_near(turn(j)).start(),
        "E": lambda j: end(turn(j)),
        "S": lambda j: along(chosen_by(j, targets)).start(),
    }

    def tick(i, carry):
        code, counts = carry
        fresh = (i % WORD) == 0
        code = jnp.where(fresh, chosen_by(i // WORD, codes), code // len(KINDS))
        kind = code % len(KINDS)
        for k, name in enumerate(KINDS[:len(doing)]):
            @pl.when(kind == k)
            def _(k=k, name=name):
                doing[name](counts[k])

        counts = tuple(count + (kind == k) for k, count in enumerate(counts))
        return code, counts

    zero = jnp.int32(0)
    lax.fori_loop(0, length, tick, (zero, (zero,) * len(KINDS)))

    numbers = lax.broadcasted_iota(jnp.int32, (2 * share, cap), 1).astype(F32)
    piece = width // 4

    def gather(e, finish):
        taking = (numbers + (e * cap).astype(F32) == slot_of).astype(F32).astype(BF16)
        for i in range(4):
            at = slice(i * piece, (i + 1) * piece)
            found = jnp.dot(taking, ret[e, :, at], preferred_element_type=F32)
            routed = rout_ref[:, at] + weights[0] * found[:share] + weights[1] * found[share:]
            if finish:
                out_ref[:, at] = (mixed_ref[:, at].astype(F32) + routed).astype(BF16)
            else:
                rout_ref[:, at] = routed

    rout_ref[...] = jnp.zeros_like(rout_ref)
    gather(z, False)

    def collect(i, carry):
        e = chosen_by(i, backs)
        home_in(e).wait_recv()
        gather(e, False)
        return carry

    lax.fori_loop(0, nz - 2, collect, 0)
    final = backs[nz - 2]
    home_in(final).wait_recv()
    gather(final, True)

    def sent(dz, carry):
        p = (z + dz) % nz
        home(p).wait_send()
        along(p).wait_send()
        return carry

    lax.fori_loop(1, nz, sent, 0)

    def sent_plane(p, carry):
        for k in range(2):
            spread(p, k).wait_send()
        forward(p).wait_send()
        hand_over(p).wait_send()
        reduce_near(p).wait_send()
        reduce_far(p).wait_send()
        return carry

    lax.fori_loop(0, nz, sent_plane, 0)
    for i in range(2):
        ho_copy(i).wait_send()
        rn_copy(i).wait_send()
        rf_copy(i).wait_send()
    for swap in swaps:
        swap.wait_send()

    @pl.when(c == 0)
    def _():
        for copy in across(s, 0):
            copy.wait_send()

    @pl.when(z + 1 < nz)
    def _():
        for copy in chain(s, 0):
            copy.wait_send()

    def sent_source(dz, carry):
        source = 2 * (z - dz) + c
        for copy in across(source, dz):
            copy.wait_send()

        @pl.when(z + 1 < nz)
        def _():
            for copy in chain(source, dz):
                copy.wait_send()

        return carry

    lax.fori_loop(1, z + 1, sent_source, 0)


def local(
    nz,
    n_tp,
    queries,
    keys,
    values,
    log_gates,
    documents,
    query_gain,
    key_gain,
    out_weight,
    residual,
    norm_gain,
    routes,
    route_weights,
    w_gate,
    w_up,
    w_down,
):
    tok_dev, heads, hd = queries.shape
    rows_dev, width = residual.shape
    n_sp = 2 * nz
    named = min(rows_dev, 6 * rows_dev // n_sp)
    cap = named + (-named) % CHUNK
    hidden_dev = w_gate.shape[2]
    extra = LIMBS * heads + LIMBS + 1
    extra = extra + (-extra) % 16
    vmem = pl.BlockSpec(memory_space=pltpu.VMEM)
    hbm = pl.BlockSpec(memory_space=pl.ANY)
    dma = pltpu.SemaphoreType.DMA
    block = (cap, width)
    smalls = (
        queries.reshape(tok_dev * heads, hd),
        keys.reshape(tok_dev, hd),
        values.reshape(tok_dev, hd),
        log_gates,
        documents[None, :],
        query_gain[None, :],
        key_gain[None, :],
        residual,
        norm_gain[None, :],
        routes.T,
        route_weights.T,
    )
    return pl.pallas_call(
        functools.partial(entry, nz, n_tp),
        out_shape=pltpu.MemorySpace.VMEM((rows_dev, width), BF16),
        in_specs=[hbm] * 15,
        out_specs=vmem,
        scratch_shapes=[pltpu.VMEM(small.shape, small.dtype) for small in smalls]
        + [
            pltpu.VMEM(out_weight.shape, BF16),
            pltpu.VMEM((2, width, hidden_dev), BF16),
            pltpu.VMEM((2, width, hidden_dev), BF16),
            pltpu.VMEM((2, hidden_dev, width), BF16),
            pltpu.VMEM((tok_dev * heads, hd), F32),
            pltpu.VMEM((2 * hd, heads * tok_dev), BF16),
            pltpu.VMEM((extra, tok_dev), F32),
            pltpu.VMEM((hd, tok_dev), F32),
            pltpu.VMEM((n_sp, tok_dev, hd), BF16),
            pltpu.VMEM((n_sp, hd + extra, tok_dev), BF16),
            pltpu.VMEM((heads, 1, tok_dev), F32),
            pltpu.VMEM((heads, 1, tok_dev), F32),
            pltpu.VMEM((heads, hd, tok_dev), F32),
            pltpu.VMEM((tok_dev, heads * hd), BF16),
            pltpu.VMEM((n_tp, rows_dev, width), BF16),
            pltpu.VMEM((2, rows_dev // 2, width), BF16),
            pltpu.VMEM((2, rows_dev, width), BF16),
            pltpu.VMEM((rows_dev, width), BF16),
            pltpu.VMEM((rows_dev, width), BF16),
            pltpu.VMEM((nz,) + block, BF16),
            pltpu.VMEM((nz, n_tp) + block, BF16),
            pltpu.VMEM((nz, n_tp) + block, BF16),
            pltpu.VMEM((nz,) + block, BF16),
            pltpu.VMEM((nz, 2) + block, BF16),
            pltpu.VMEM((nz,) + block, BF16),
            pltpu.VMEM((nz,) + block, BF16),
            pltpu.VMEM((rows_dev, width), F32),
            dma((4,)),
            dma((3,)),
            dma((3,)),
            dma((nz,)),
            dma((nz,)),
            dma((nz,)),
            dma((nz,)),
            dma((n_sp,)),
            dma((n_sp,)),
            dma((2,)),
            dma((2,)),
            dma((2,)),
            dma((2,)),
            dma((2,)),
            dma((2,)),
            dma((nz,)),
            dma((nz,)),
            dma((2, nz)),
            dma((2, nz)),
            dma((nz,)),
            dma((nz,)),
            dma((nz,)),
            dma((nz,)),
            dma((2, nz)),
            dma((2, nz)),
            dma((nz,)),
            dma((nz,)),
            dma((len(smalls),)),
        ],
        compiler_params=pltpu.CompilerParams(
            collective_id=0, has_side_effects=True, vmem_limit_bytes=60 * 1024 * 1024
        ),
        name="layer",
    )(*smalls[:7], out_weight, *smalls[7:], w_gate[0], w_up[0], w_down[0])


def solution(mesh):
    return jax.shard_map(
        functools.partial(local, mesh.shape["sp"] // 2, mesh.shape["tp"]),
        mesh=mesh,
        in_specs=(
            P(("grp", "sp"), "tp", None),
            P(("grp", "sp"), "tp", None),
            P(("grp", "sp"), "tp", None),
            P("tp", ("grp", "sp")),
            P(("grp", "sp")),
            P(),
            P(),
            P("tp", None),
            P(("grp", "sp", "tp"), None),
            P(),
            P(("grp", "sp", "tp"), None),
            P(("grp", "sp", "tp"), None),
            P("sp", None, "tp"),
            P("sp", None, "tp"),
            P("sp", "tp", None),
        ),
        out_specs=P(("grp", "sp", "tp"), None),
        check_vma=False,
    )
```

```python
import functools

import jax
import jax.numpy as jnp
from jax import lax
from jax.experimental import pallas as pl
from jax.experimental.pallas import tpu as pltpu
from jax.sharding import PartitionSpec as P

EPSILON = 1e-06
CHUNK = 16
LIMBS = 3
MESH = pl.DeviceIdType.MESH
BF16 = jnp.bfloat16
F32 = jnp.float32


def rms_scale(inputs, gain):
    return inputs * lax.rsqrt(jnp.mean(inputs * inputs, axis=-1, keepdims=True) + EPSILON) * gain


def flip(index, bits, size):
    step = 1
    while step < size:
        bit = (bits // step) % 2
        index = index + bit * step * (1 - 2 * ((index // step) % 2))
        step *= 2
    return index


def remote(src, dst, send, recv, where):
    return pltpu.make_async_remote_copy(
        src, dst, send, recv, device_id=where, device_id_type=MESH
    )


KINDS = "LFCDRESN"
WORD = 10
PLANS = (
    ("SLFLSCFSLCFLDRFCDRCEDREDREE", "0123", "0123", "123", "123"),
    ("SLFLSCFSLCFLDRFCDRCEDREDREE", "0123", "0123", "123", "123"),
    ("SSLLFSFLFCRLFCRDCDEDRECEDRE", "1023", "0231", "023", "023"),
    ("SSLLFSFLFCRLFCRDCDEDRECEDRE", "1023", "0231", "023", "023"),
    ("SSSLLFFLLFCRFCRDCDEDRECEDRE", "2103", "1032", "310", "103"),
    ("SSSLLFFLLFCRFCRDCDEDRECEDRE", "2103", "1032", "310", "103"),
    ("SLLFSFSLLFCRFCRDCDECDREDREE", "3201", "2013", "201", "012"),
    ("SLLFSFSLLFCRFCRDCDECDREDREE", "3201", "2013", "201", "012"),
)


def plan(nz, s):
    if 2 * nz == len(PLANS):
        text, *lists = PLANS[s]
        return [text] + [[int(plane) for plane in planes] for planes in lists]
    z = s // 2
    text = "S" * (nz - 1) + "L" + "FL" * (nz - 1) + "F" + "CRD" * nz + "E" * nz
    planes = [(z + dz) % nz for dz in range(nz)]
    return [text, planes, planes[1:] + planes[:1], planes[1:], planes[1:]]


def packed(text):
    words = []
    for at in range(0, len(text), WORD):
        word = 0
        for kind in reversed(text[at:at + WORD]):
            word = word * len(KINDS) + KINDS.index(kind)
        words.append(word)
    return words


def chosen_by(index, values):
    total = 0
    for i, value in enumerate(values):
        total = total + (index == i) * value
    return total


def entry(nz, n_tp, *refs):
    small = refs[:7] + refs[8:12]
    held = refs[16:16 + len(small)]
    fills = [
        pltpu.make_async_copy(src, dst, refs[-1].at[i])
        for i, (src, dst) in enumerate(zip(small, held))
    ]
    layer_kernel(
        nz, n_tp, fills, *held[:7], refs[7], *held[7:], *refs[12:16],
        *refs[16 + len(small):-1],
    )


def layer_kernel(
    nz,
    n_tp,
    fills,
    q_ref,
    k_ref,
    v_ref,
    g_ref,
    d_ref,
    qg_ref,
    kg_ref,
    w_hbm,
    res_ref,
    gain_ref,
    rt_ref,
    rw_ref,
    wg_hbm,
    wu_hbm,
    wd_hbm,
    out_ref,
    w_ref,
    wg_ref,
    wu_ref,
    wd_ref,
    qf_ref,
    qt_ref,
    ext_ref,
    kx_ref,
    k_buf,
    v_buf,
    m_ref,
    l_ref,
    acc_ref,
    att_ref,
    sbuf,
    pho_buf,
    prs_buf,
    mixed_ref,
    normed_ref,
    out_buf,
    arrived,
    part,
    hbuf,
    rbuf,
    fin,
    ret,
    rout_ref,
    w_sem,
    wx_send,
    wx_recv,
    kc_send,
    vc_send,
    kx_send,
    vx_send,
    k_recv,
    v_recv,
    pho_send,
    pho_recv,
    prn_send,
    prn_recv,
    prf_send,
    prf_recv,
    a_send,
    a_recv,
    b_send,
    b_recv,
    f_send,
    f_recv,
    h_send,
    h_recv,
    r_send,
    r_recv,
    z_send,
    z_recv,
):
    s = lax.axis_index("sp")
    t = lax.axis_index("tp")
    z, c = s // 2, s % 2
    heads, rows, hd = acc_ref.shape[0], acc_ref.shape[2], acc_ref.shape[1]
    extra = ext_ref.shape[0]
    cap, width = out_buf.shape[1:]
    share = rows // n_tp
    half = share // 2
    partner = {"sp": 2 * z + 1 - c}
    near = 1 + c
    far = 2 - c
    near_at = flip(t, near, n_tp)
    far_at = flip(t, far, n_tp)
    to_near = {"tp": near_at}
    to_far = {"tp": far_at}

    barrier = pltpu.get_barrier_semaphore()
    for dz in range(1, nz):
        pl.semaphore_signal(
            barrier, inc=1, device_id={"sp": 2 * ((z + dz) % nz) + c}, device_id_type=MESH
        )
    for k in (1, 2):
        pl.semaphore_signal(
            barrier, inc=1, device_id={"tp": flip(t, k, n_tp)}, device_id_type=MESH
        )
    pl.semaphore_signal(barrier, inc=1, device_id=partner, device_id_type=MESH)
    loads = [
        pltpu.make_async_copy(src, dst, w_sem.at[i])
        for i, (src, dst) in enumerate(
            (
                (w_hbm, w_ref),
                (wg_hbm, wg_ref.at[0]),
                (wu_hbm, wu_ref.at[0]),
                (wd_hbm, wd_ref.at[0]),
            )
        )
    ]
    first = (1, 2, 3, 4, 6)
    for i in first:
        fills[i].start()
    for i, fill in enumerate(fills):
        if i not in first:
            fill.start()
    swaps = [
        remote(src, dst, wx_send.at[i], wx_recv.at[i], partner)
        for i, (src, dst) in enumerate(
            ((wg_hbm, wg_ref.at[1]), (wu_hbm, wu_ref.at[1]), (wd_hbm, wd_ref.at[1]))
        )
    ]

    for i in first:
        fills[i].wait()
    k_buf[s] = rms_scale(k_ref[...].astype(F32), kg_ref[...]).astype(BF16)
    v_buf[s, 0:hd, :] = jnp.transpose(v_ref[...])
    gates = -g_ref[...]
    high = gates.astype(BF16).astype(F32)
    middle = (gates - high).astype(BF16).astype(F32)
    low = (gates - high - middle).astype(BF16).astype(F32)
    limbs = (high, middle, low)
    ext_ref[...] = jnp.zeros_like(ext_ref)
    for j, limb in enumerate(limbs):
        ext_ref[j * heads:(j + 1) * heads, :] = limb
    ones_at = LIMBS * heads
    doc_at = ones_at + LIMBS
    ext_ref[ones_at:ones_at + LIMBS, :] = jnp.ones((LIMBS, rows), F32)
    ext_ref[doc_at:doc_at + 1, :] = d_ref[...].astype(F32)
    v_buf[s, hd:hd + extra, :] = ext_ref[...].astype(BF16)

    pl.semaphore_wait(barrier, nz - 1 + 2 + 1)

    def chain(source, slot):
        there = {"sp": 2 * (z + 1) + c}
        return (
            remote(
                k_buf.at[source], k_buf.at[source], kc_send.at[slot], k_recv.at[source], there
            ),
            remote(
                v_buf.at[source], v_buf.at[source], vc_send.at[slot], v_recv.at[source], there
            ),
        )

    def across(source, slot):
        return (
            remote(
                k_buf.at[source], k_buf.at[source], kx_send.at[slot], k_recv.at[source], partner
            ),
            remote(
                v_buf.at[source], v_buf.at[source], vx_send.at[slot], v_recv.at[source], partner
            ),
        )

    @pl.when(z + 1 < nz)
    def _():
        for copy in chain(s, 0):
            copy.start()

    @pl.when(c == 0)
    def _():
        for copy in across(s, 0):
            copy.start()

    for i, fill in enumerate(fills):
        if i not in first:
            fill.wait()
    for load in loads:
        load.start()

    qf_ref[...] = q_ref[...].astype(F32)
    row = lax.broadcasted_iota(jnp.int32, (extra, rows), 0)
    for h in range(heads):
        picked = qf_ref[pl.ds(h, rows, stride=heads), :]
        query = (rms_scale(picked, qg_ref[...]) * hd ** (-0.5)).astype(BF16).astype(F32)
        lanes = slice(h * rows, (h + 1) * rows)
        qt_ref[0:hd, lanes] = jnp.transpose(query).astype(BF16)
        mine = jnp.where((row < ones_at) & (row % heads == h), 1.0, 0.0)
        for j, limb in enumerate(limbs):
            mine = jnp.where(row == ones_at + j, -limb[h:h + 1, :], mine)
        qt_ref[hd:hd + extra, lanes] = mine.astype(BF16)
        qt_ref[hd + extra:, lanes] = jnp.zeros((hd - extra, rows), BF16)
    kx_ref[...] = jnp.zeros_like(kx_ref)
    here = d_ref[...].astype(F32)

    def update(source, own):
        kx_ref[0:extra, :] = v_buf[source, hd:hd + extra, :].astype(F32)
        columns = jnp.transpose(kx_ref[...])
        left = jnp.concatenate([k_buf[source], columns.astype(BF16)], axis=1)
        same = columns[:, doc_at:doc_at + 1] == here
        if own:
            key_at = lax.broadcasted_iota(jnp.int32, (rows, rows), 0)
            query_at = lax.broadcasted_iota(jnp.int32, (rows, rows), 1)
            same = same & (key_at <= query_at)
        products = jnp.dot(left, qt_ref[...], preferred_element_type=F32)
        expos = []
        factors = []
        for h in range(heads):
            scores = jnp.where(same, products[:, h * rows:(h + 1) * rows], -jnp.inf)
            peak = jnp.max(scores, axis=0, keepdims=True)
            if own:
                new = peak
            else:
                old = m_ref[h]
                new = jnp.maximum(old, peak)
                factors.append(jnp.exp(old - new))
            expo = jnp.exp(scores - new)
            total = jnp.sum(expo, axis=0, keepdims=True)
            m_ref[h] = new
            l_ref[h] = total if own else factors[h] * l_ref[h] + total
            expos.append(expo.astype(BF16))
        mixes = jnp.dot(
            v_buf[source, 0:hd, :],
            jnp.concatenate(expos, axis=1),
            preferred_element_type=F32,
        )
        for h in range(heads):
            mix = mixes[:, h * rows:(h + 1) * rows]
            acc_ref[h] = mix if own else factors[h] * acc_ref[h] + mix

    update(s, True)

    def one_source(i, carry):
        dz = (i + 1) // 2
        direct = i % 2
        core = (1 - direct) * (1 - c) + direct * c
        source = 2 * (z - dz) + core
        onward = chain(source, dz)
        aside = across(source, dz)
        for k in range(2):
            aside[k].wait_recv()

            @pl.when(direct == 1)
            def _(k=k):
                @pl.when(z + 1 < nz)
                def _():
                    onward[k].start()

                aside[k].start()

        update(source, False)
        return carry

    lax.fori_loop(1 - c, 2 * z + 1, one_source, 0)

    for swap in swaps:
        swap.start()

    for h in range(heads):
        att_ref[:, h * hd:(h + 1) * hd] = jnp.transpose((acc_ref[h] * (1.0 / l_ref[h])).astype(BF16))

    def ho_copy(i):
        return remote(
            sbuf.at[3, pl.ds(i * half, half)], pho_buf.at[i], pho_send.at[i], pho_recv.at[i],
            to_near,
        )

    def rn_copy(i):
        return remote(
            sbuf.at[near, pl.ds(i * half, half)], prs_buf.at[0, pl.ds(i * half, half)],
            prn_send.at[i], prn_recv.at[i], to_near,
        )

    def rf_copy(i):
        return remote(
            sbuf.at[far, pl.ds(i * half, half)], prs_buf.at[1, pl.ds(i * half, half)],
            prf_send.at[i], prf_recv.at[i], to_far,
        )

    loads[0].wait()

    def project(k, column):
        start = pl.multiple_of(column * share, share)
        block = jnp.dot(
            att_ref[pl.ds(start, share), :], w_ref[...], preferred_element_type=F32
        )
        sbuf[k] = block.astype(BF16)

    def project_step(i, carry):
        k = (i == 0) * 3 + (i == 1) * near + (i == 2) * far
        project(k, flip(t, k, n_tp))

        @pl.when(i == 0)
        def _():
            for j in range(2):
                ho_copy(j).start()

        @pl.when(i == 1)
        def _():
            for j in range(2):
                rn_copy(j).start()

        return carry

    lax.fori_loop(0, n_tp, project_step, 0)

    for i in range(2):
        ho_copy(i).wait_recv()

        def pair(r, carry, i=i):
            at = pl.ds(pl.multiple_of(i * half + r * CHUNK, CHUNK), CHUNK)
            here_at = pl.ds(pl.multiple_of(r * CHUNK, CHUNK), CHUNK)
            total = sbuf[far, at, :].astype(F32) + pho_buf[i, here_at, :].astype(F32)
            sbuf[far, at, :] = total.astype(BF16)
            return carry

        lax.fori_loop(0, half // CHUNK, pair, 0)
        rf_copy(i).start()

    experts = nz
    padded = experts + (-experts) % 8
    n_slots = experts * cap
    first, second = rt_ref[0:1, :], rt_ref[1:2, :]
    names = lax.broadcasted_iota(jnp.int32, (padded, share), 0)
    chosen = [(names == first).astype(F32), (names == second).astype(F32)]
    up_to = lax.broadcasted_iota(jnp.int32, (share, share), 0) <= lax.broadcasted_iota(
        jnp.int32, (share, share), 1
    )
    rank = (
        jnp.dot(
            (chosen[0] + chosen[1]).astype(BF16),
            up_to.astype(F32).astype(BF16),
            preferred_element_type=F32,
        )
        - 1.0
    )
    start_of = names.astype(F32) * cap
    slots = [
        jnp.sum(choice * (rank + start_of), axis=0, keepdims=True) for choice in chosen
    ]
    slot_rows = lax.broadcasted_iota(jnp.int32, (n_slots, share), 0).astype(F32)
    placing = (
        (slot_rows == slots[0]).astype(F32) + (slot_rows == slots[1]).astype(F32)
    ).astype(BF16)
    diagonal = (
        lax.broadcasted_iota(jnp.int32, (share, share), 0)
        == lax.broadcasted_iota(jnp.int32, (share, share), 1)
    ).astype(F32)

    def column(values):
        return jnp.sum(diagonal * values, axis=1, keepdims=True)

    slot_of = jnp.concatenate([column(slot) for slot in slots], axis=0)
    weights = [column(rw_ref[k:k + 1, :]) for k in range(2)]

    for i in range(2):
        rn_copy(i).wait_recv()
        rf_copy(i).wait_recv()

        def finish(r, carry, i=i):
            at = pl.ds(pl.multiple_of(i * half + r * CHUNK, CHUNK), CHUNK)
            total = (
                sbuf[0, at, :].astype(F32)
                + prs_buf[0, at, :].astype(F32)
                + prs_buf[1, at, :].astype(F32)
            )
            mixed = (res_ref[at, :].astype(F32) + total).astype(BF16)
            mixed_ref[at, :] = mixed
            normed_ref[at, :] = rms_scale(mixed.astype(F32), gain_ref[...]).astype(BF16)
            return carry

        lax.fori_loop(0, half // CHUNK, finish, 0)

    out_buf[...] = (
        jnp.dot(placing, normed_ref[...], preferred_element_type=F32)
        .astype(BF16)
        .reshape(experts, cap, width)
    )

    plans = [plan(nz, i) for i in range(2 * nz)]
    longest = max(len(text) for text, *_ in plans)
    codes = [packed(text) for text, *_ in plans]
    codes = [
        chosen_by(s, [words[i] if i < len(words) else 0 for words in codes])
        for i in range(-(-longest // WORD))
    ]
    length = chosen_by(s, [len(text) for text, *_ in plans])
    orders, turns, targets, backs = (
        [chosen_by(s, planes) for planes in zip(*lists)]
        for lists in list(zip(*plans))[1:]
    )

    def order(j):
        return chosen_by(j, orders)

    def turn(j):
        return chosen_by(j, turns)

    def along(e):
        return remote(
            out_buf.at[e], arrived.at[z, t], a_send.at[e], a_recv.at[z], {"sp": 2 * e + c}
        )

    def along_in(p):
        return remote(
            arrived.at[p, t], arrived.at[p, t], a_send.at[p], a_recv.at[p], partner
        )

    def spread(p, k):
        block = arrived.at[p, t]
        return remote(
            block, block, b_send.at[k, p], b_recv.at[k, p], to_far if k else to_near
        )

    def spread_in(p, k):
        block = arrived.at[p, far_at if k else near_at]
        return remote(block, block, b_send.at[k, p], b_recv.at[k, p], partner)

    def forward(p):
        block = arrived.at[p, far_at]
        return remote(block, block, f_send.at[p], f_recv.at[p], to_near)

    def forward_in(p):
        block = arrived.at[p, flip(t, 3, n_tp)]
        return remote(block, block, f_send.at[p], f_recv.at[p], partner)

    def hand_over(p):
        return remote(
            part.at[p, flip(t, 3, n_tp)], hbuf.at[p], h_send.at[p], h_recv.at[p], to_near
        )

    def reduce_near(p):
        return remote(
            part.at[p, near_at], rbuf.at[p, 0], r_send.at[0, p], r_recv.at[0, p], to_near
        )

    def reduce_far(p):
        return remote(
            part.at[p, far_at], rbuf.at[p, 1], r_send.at[1, p], r_recv.at[1, p], to_far
        )

    def home(p):
        return remote(
            fin.at[p], ret.at[z], z_send.at[p], z_recv.at[z], {"sp": 2 * p + c}
        )

    def home_in(e):
        return remote(fin.at[e], ret.at[e], z_send.at[e], z_recv.at[e], partner)

    def launch(p):
        @pl.when(p != z)
        def _():
            along_in(p).wait_recv()

        spread(p, 0).start()
        spread(p, 1).start()

    arrived[z, t] = out_buf[z]

    def pass_on(p):
        spread_in(p, 1).wait_recv()
        forward(p).start()

    for load in loads[1:]:
        load.wait()

    def compute(p, index):
        @pl.when(index == 0)
        def _():
            for swap in swaps:
                swap.wait_recv()

        spread_in(p, 0).wait_recv()
        forward_in(p).wait_recv()
        flat = arrived[p].reshape(n_tp * cap, width)
        result = None
        for i in range(2):
            gate = jnp.dot(flat, wg_ref[i], preferred_element_type=F32)
            up = jnp.dot(flat, wu_ref[i], preferred_element_type=F32)
            hidden = (gate * (1.0 / (1.0 + jnp.exp(-gate))) * up).astype(BF16)
            down = jnp.dot(hidden, wd_ref[i], preferred_element_type=F32)
            result = down if result is None else result + down
        part[p] = result.astype(BF16).reshape(n_tp, cap, width)
        hand_over(p).start()

    def add_far(p):
        hand_over(p).wait_recv()

        def one(r, carry):
            at = pl.ds(pl.multiple_of(r * CHUNK, CHUNK), CHUNK)
            total = part[p, far_at, at, :].astype(F32) + hbuf[p, at, :].astype(F32)
            part[p, far_at, at, :] = total.astype(BF16)
            return carry

        lax.fori_loop(0, cap // CHUNK, one, 0)
        reduce_far(p).start()

    def end(p):
        reduce_near(p).wait_recv()
        reduce_far(p).wait_recv()

        def one(r, carry):
            at = pl.ds(pl.multiple_of(r * CHUNK, CHUNK), CHUNK)
            total = (
                part[p, t, at, :].astype(F32)
                + rbuf[p, 0, at, :].astype(F32)
                + rbuf[p, 1, at, :].astype(F32)
            )
            fin[p, at, :] = total.astype(BF16)
            return carry

        lax.fori_loop(0, cap // CHUNK, one, 0)

        @pl.when(p != z)
        def _():
            home(p).start()

        @pl.when(p == z)
        def _():
            ret[z] = fin[z]

    doing = {
        "L": lambda j: launch(order(j)),
        "F": lambda j: pass_on(order(j)),
        "C": lambda j: compute(turn(j), j),
        "D": lambda j: add_far(turn(j)),
        "R": lambda j: reduce_near(turn(j)).start(),
        "E": lambda j: end(turn(j)),
        "S": lambda j: along(chosen_by(j, targets)).start(),
    }

    def tick(i, carry):
        code, counts = carry
        fresh = (i % WORD) == 0
        code = jnp.where(fresh, chosen_by(i // WORD, codes), code // len(KINDS))
        kind = code % len(KINDS)
        for k, name in enumerate(KINDS[:len(doing)]):
            @pl.when(kind == k)
            def _(k=k, name=name):
                doing[name](counts[k])

        counts = tuple(count + (kind == k) for k, count in enumerate(counts))
        return code, counts

    zero = jnp.int32(0)
    lax.fori_loop(0, length, tick, (zero, (zero,) * len(KINDS)))

    numbers = lax.broadcasted_iota(jnp.int32, (2 * share, cap), 1).astype(F32)
    piece = width // 4

    def gather(e, finish):
        taking = (numbers + (e * cap).astype(F32) == slot_of).astype(F32).astype(BF16)
        for i in range(4):
            at = slice(i * piece, (i + 1) * piece)
            found = jnp.dot(taking, ret[e, :, at], preferred_element_type=F32)
            routed = rout_ref[:, at] + weights[0] * found[:share] + weights[1] * found[share:]
            if finish:
                out_ref[:, at] = (mixed_ref[:, at].astype(F32) + routed).astype(BF16)
            else:
                rout_ref[:, at] = routed

    rout_ref[...] = jnp.zeros_like(rout_ref)
    gather(z, False)

    def collect(i, carry):
        e = chosen_by(i, backs)
        home_in(e).wait_recv()
        gather(e, False)
        return carry

    lax.fori_loop(0, nz - 2, collect, 0)
    final = backs[nz - 2]
    home_in(final).wait_recv()
    gather(final, True)

    def sent(dz, carry):
        p = (z + dz) % nz
        home(p).wait_send()
        along(p).wait_send()
        return carry

    lax.fori_loop(1, nz, sent, 0)

    def sent_plane(p, carry):
        for k in range(2):
            spread(p, k).wait_send()
        forward(p).wait_send()
        hand_over(p).wait_send()
        reduce_near(p).wait_send()
        reduce_far(p).wait_send()
        return carry

    lax.fori_loop(0, nz, sent_plane, 0)
    for i in range(2):
        ho_copy(i).wait_send()
        rn_copy(i).wait_send()
        rf_copy(i).wait_send()
    for swap in swaps:
        swap.wait_send()

    @pl.when(c == 0)
    def _():
        for copy in across(s, 0):
            copy.wait_send()

    @pl.when(z + 1 < nz)
    def _():
        for copy in chain(s, 0):
            copy.wait_send()

    def sent_source(dz, carry):
        source = 2 * (z - dz) + c
        for copy in across(source, dz):
            copy.wait_send()

        @pl.when(z + 1 < nz)
        def _():
            for copy in chain(source, dz):
                copy.wait_send()

        return carry

    lax.fori_loop(1, z + 1, sent_source, 0)


def local(
    nz,
    n_tp,
    queries,
    keys,
    values,
    log_gates,
    documents,
    query_gain,
    key_gain,
    out_weight,
    residual,
    norm_gain,
    routes,
    route_weights,
    w_gate,
    w_up,
    w_down,
):
    tok_dev, heads, hd = queries.shape
    rows_dev, width = residual.shape
    n_sp = 2 * nz
    named = min(rows_dev, 6 * rows_dev // n_sp)
    cap = named + (-named) % CHUNK
    hidden_dev = w_gate.shape[2]
    extra = LIMBS * heads + LIMBS + 1
    extra = extra + (-extra) % 16
    vmem = pl.BlockSpec(memory_space=pltpu.VMEM)
    hbm = pl.BlockSpec(memory_space=pl.ANY)
    dma = pltpu.SemaphoreType.DMA
    block = (cap, width)
    smalls = (
        queries.reshape(tok_dev * heads, hd),
        keys.reshape(tok_dev, hd),
        values.reshape(tok_dev, hd),
        log_gates,
        documents[None, :],
        query_gain[None, :],
        key_gain[None, :],
        residual,
        norm_gain[None, :],
        routes.T,
        route_weights.T,
    )
    return pl.pallas_call(
        functools.partial(entry, nz, n_tp),
        out_shape=pltpu.MemorySpace.VMEM((rows_dev, width), BF16),
        in_specs=[hbm] * 15,
        out_specs=vmem,
        scratch_shapes=[pltpu.VMEM(small.shape, small.dtype) for small in smalls]
        + [
            pltpu.VMEM(out_weight.shape, BF16),
            pltpu.VMEM((2, width, hidden_dev), BF16),
            pltpu.VMEM((2, width, hidden_dev), BF16),
            pltpu.VMEM((2, hidden_dev, width), BF16),
            pltpu.VMEM((tok_dev * heads, hd), F32),
            pltpu.VMEM((2 * hd, heads * tok_dev), BF16),
            pltpu.VMEM((extra, tok_dev), F32),
            pltpu.VMEM((hd, tok_dev), F32),
            pltpu.VMEM((n_sp, tok_dev, hd), BF16),
            pltpu.VMEM((n_sp, hd + extra, tok_dev), BF16),
            pltpu.VMEM((heads, 1, tok_dev), F32),
            pltpu.VMEM((heads, 1, tok_dev), F32),
            pltpu.VMEM((heads, hd, tok_dev), F32),
            pltpu.VMEM((tok_dev, heads * hd), BF16),
            pltpu.VMEM((n_tp, rows_dev, width), BF16),
            pltpu.VMEM((2, rows_dev // 2, width), BF16),
            pltpu.VMEM((2, rows_dev, width), BF16),
            pltpu.VMEM((rows_dev, width), BF16),
            pltpu.VMEM((rows_dev, width), BF16),
            pltpu.VMEM((nz,) + block, BF16),
            pltpu.VMEM((nz, n_tp) + block, BF16),
            pltpu.VMEM((nz, n_tp) + block, BF16),
            pltpu.VMEM((nz,) + block, BF16),
            pltpu.VMEM((nz, 2) + block, BF16),
            pltpu.VMEM((nz,) + block, BF16),
            pltpu.VMEM((nz,) + block, BF16),
            pltpu.VMEM((rows_dev, width), F32),
            dma((4,)),
            dma((3,)),
            dma((3,)),
            dma((nz,)),
            dma((nz,)),
            dma((nz,)),
            dma((nz,)),
            dma((n_sp,)),
            dma((n_sp,)),
            dma((2,)),
            dma((2,)),
            dma((2,)),
            dma((2,)),
            dma((2,)),
            dma((2,)),
            dma((nz,)),
            dma((nz,)),
            dma((2, nz)),
            dma((2, nz)),
            dma((nz,)),
            dma((nz,)),
            dma((nz,)),
            dma((nz,)),
            dma((2, nz)),
            dma((2, nz)),
            dma((nz,)),
            dma((nz,)),
            dma((len(smalls),)),
        ],
        compiler_params=pltpu.CompilerParams(
            collective_id=0, has_side_effects=True, vmem_limit_bytes=60 * 1024 * 1024
        ),
        name="layer",
    )(*smalls[:7], out_weight, *smalls[7:], w_gate[0], w_up[0], w_down[0])


def solution(mesh):
    return jax.shard_map(
        functools.partial(local, mesh.shape["sp"] // 2, mesh.shape["tp"]),
        mesh=mesh,
        in_specs=(
            P(("grp", "sp"), "tp", None),
            P(("grp", "sp"), "tp", None),
            P(("grp", "sp"), "tp", None),
            P("tp", ("grp", "sp")),
            P(("grp", "sp")),
            P(),
            P(),
            P("tp", None),
            P(("grp", "sp", "tp"), None),
            P(),
            P(("grp", "sp", "tp"), None),
            P(("grp", "sp", "tp"), None),
            P("sp", None, "tp"),
            P("sp", None, "tp"),
            P("sp", "tp", None),
        ),
        out_specs=P(("grp", "sp", "tp"), None),
        check_vma=False,
    )
```
